128 devices in a mesh: sp: 32 (over z, y, core), tp: 4 (over x).
Axes of the slice: x: 4, y: 4, z: 4, core: 2. Of those that a mesh axis runs over, the one named last changes fastest.
Arguments:
- residual: bfloat16 [16384, 2048], P(('sp', 'tp')), may hold values from -6 to 6
- query_proj: bfloat16 [16384, 2048], P('sp', 'tp'), may hold values from -12 to 12
- key_proj: bfloat16 [16384, 512], P('sp', 'tp'), may hold values from -12 to 12
- value_proj: bfloat16 [16384, 512], P('sp', 'tp'), may hold values from -6 to 6
- query_gain: float32 [128], replicated, may hold values from 0.4 to 4.5
- key_gain: float32 [128], replicated, may hold values from 0.4 to 4.5
- document_ids: int32 [16384], P('sp'), may hold values from 0 to 15, never falling along the last dimension, each value on 1 to 1537 neighbouring positions
- output_weight: bfloat16 [2048, 2048], replicated, may hold values from -0.125 to 0.125
- norm_gain: float32 [2048], replicated, may hold values from 0.1 to 1.9
- expert_ids: int32 [16384, 2], P(('sp', 'tp')), may hold values from 0 to 127, all different within a row; in each aligned block of 128 rows (0 to 127, 128 to 255, ...) at most 4 rows name the same one
- route_weights: float32 [16384, 2], P(('sp', 'tp')), may hold values from 0.2 to 1
- gate_weight: bfloat16 [128, 2048, 512], P(('sp', 'tp')), may hold values from -0.125 to 0.125
- up_weight: bfloat16 [128, 2048, 512], P(('sp', 'tp')), may hold values from -0.125 to 0.125
- down_weight: bfloat16 [128, 512, 2048], P(('sp', 'tp')), may hold values from -0.25 to 0.25
Outputs:
- updated: bfloat16 [16384, 2048], P(('sp', 'tp'))
The draws below stay inside these ranges and needn't reach their ends.
Inputs may be any that keep to these rules, and one draw needn't show every extreme that they name: `document_ids`: document numbers never fall along the positions; each document has at most 1537 positions, and one has exactly 1537. `expert_ids`: each row names 2 different experts; within the rows of one device no expert is named more than 4 times, and in some device's rows an expert is named exactly 4 times.
All inputs are finite; a program needn't handle non-finite values.
Results may differ from the reference program's by a relative error of at most 0.017.
Values may be sent and summed in bfloat16 or wider, within the bound.
No kernel may reach another device: no remote copies, remote signals or barrier semaphores. Data moves between devices by JAX's collectives and lax.ppermute only.
A program may use at most 128 MiB of HBM per device.

```python
import math
import jax
import jax.numpy as jnp
import numpy as np
from jax import lax

D = 2048
HEADS = 16
KV_HEADS = 4
HEAD = 128
GRID_W = 64
FFE = 512
TOPK = 2
REACH = 3
TOK_DEV = 512
TOKENS = 16384
EROWS = 128
EXPERTS = 128
CAP = 4
DOC_MOST = 1537
DOCS = 16
N_SP = 32
N_TP = 4


def drawn(key):
    base = jax.random.fold_in(key, 7)
    key_q, key_k, key_g = jax.random.split(base, 3)
    queries = jnp.clip(jax.random.normal(key_q, (TOKENS, HEADS * HEAD), jnp.float32), -6.0, 6.0)
    keys = jnp.clip(jax.random.normal(key_k, (TOKENS, KV_HEADS * HEAD), jnp.float32), -6.0, 6.0)
    gains = jnp.exp(jax.random.uniform(key_g, (2, HEAD), jnp.float32, -0.7, 0.7))
    return (queries, keys, gains)


def draw_query_proj(key, part):
    return drawn(key)[0].astype(jnp.bfloat16)


def draw_key_proj(key, part):
    return drawn(key)[1].astype(jnp.bfloat16)


def draw_query_gain(key, part):
    return drawn(key)[2][0]


def draw_key_gain(key, part):
    return drawn(key)[2][1]


def levels(key, shape, shards, low, high):
    gain = 1.0
    for dim, parts in shards:
        heights = jax.random.uniform(jax.random.fold_in(jax.random.fold_in(key, 6), dim), (parts,), jnp.float32, low / len(shards), high / len(shards))
        gain = gain * jnp.repeat(jnp.exp(heights), shape[dim] // parts).reshape((-1,) + (1,) * (len(shape) - 1 - dim))
    return gain


def length_profile(number_of, total, most, skew):
    weights = [(1 << 20) // math.isqrt(grade ** skew) + 1 for grade in range(2, number_of + 1)]
    spare, given = total - most - (number_of - 1), [1] * (number_of - 1)
    while spare > 0:
        movable = [i for i in range(number_of - 1) if given[i] < most]
        mass, budget = sum([weights[i] for i in movable]), spare
        for i in movable:
            extra = min(most - given[i], max(1, budget * weights[i] // mass), spare)
            given[i] = given[i] + extra
            spare = spare - extra
    return np.array([most] + given)


def uneven(own_key, number_of, total, bound, skew):
    if number_of == 2:
        one = jax.random.randint(own_key, (), max(1, total - bound), min(bound, total - 1) + 1)
        return jnp.stack([one, total - one])
    lengths = jnp.asarray(length_profile(number_of, total, bound, skew), jnp.int32)
    twos = (number_of - 1) // 2
    donor, receiver = lengths[1:1 + 2 * twos:2], lengths[2:2 + 2 * twos:2]
    slack = jnp.minimum(donor - 1, bound - receiver)
    shifted = jax.random.randint(jax.random.fold_in(own_key, 1), (twos,), 0, 1 << 20) % (slack + 1)
    lengths = lengths.at[1:1 + 2 * twos:2].set(donor - shifted).at[2:2 + 2 * twos:2].set(receiver + shifted)
    return lengths[jax.random.permutation(jax.random.fold_in(own_key, 2), number_of)]


def assign_block(stream_key, own, number, rows, number_of, top, reach, lean):
    order = jax.random.permutation(stream_key, number_of)
    packed, common = shares(number_of, rows * top, reach, lean, True), shares(number_of, rows * top, reach, lean, False)
    places = jnp.arange(number_of)

    def named(tallies, offset_by):
        used = int((tallies > 0).sum())
        fixed = max(1, used // 4)
        shifted = fixed + (places - fixed + offset_by * (used - fixed)) % max(1, number_of - fixed)
        return jnp.zeros((number_of,), jnp.int32).at[order[jnp.where(places < fixed, places, shifted)]].set(jnp.asarray(tallies, jnp.int32))

    tallies = jnp.where(number % 4 == 0, named(packed, number // 4), named(common, number - number // 4 - 1))
    mixed = jax.random.permutation(jax.random.fold_in(own, 3), number_of)
    source_of, taker = mixed[0:number_of // 2 * 2:2], mixed[1:number_of // 2 * 2:2]
    room = jnp.minimum(tallies[source_of] - 1, reach - tallies[taker]) // 2
    room = jnp.where((source_of == order[0]) | (taker == order[0]) | (tallies[taker] == 0), 0, jnp.maximum(room, 0))
    shifted = jax.random.randint(jax.random.fold_in(own, 4), (number_of // 2,), 0, 1 << 20) % (room + 1)
    tallies = tallies.at[source_of].add(-shifted).at[taker].add(shifted)
    members = jnp.searchsorted(jnp.cumsum(tallies), jnp.arange(rows * top), side="right").astype(jnp.int32)
    table = members.reshape(top, rows).T
    table = table[jax.random.permutation(jax.random.fold_in(own, 1), rows)]
    offset_by = jax.random.randint(jax.random.fold_in(own, 2), (rows, 1), 0, top)
    return jnp.take_along_axis(table, (jnp.arange(top)[None, :] + offset_by) % top, axis=1)


def shares(number_of, total, most, lean, full):
    portions = [(1 << 20) // math.isqrt(standing ** lean) + 1 for standing in range(1, number_of + 1)]
    largest = most if full else min(most, max(-(-total // number_of), total * portions[0] // sum(portions)))
    least = 1 if total - largest >= number_of - 1 else 0
    given, surplus = [largest] + [least] * (number_of - 1), total - largest - least * (number_of - 1)
    while surplus > 0:
        candidates = [i for i in range(1, number_of) if given[i] < largest] or [i for i in range(1, number_of) if given[i] < most]
        whole, remaining = sum([portions[i] for i in candidates]), surplus
        for i in candidates:
            extra = min(most - given[i], max(1, remaining * portions[i] // whole), surplus)
            given[i] = given[i] + extra
            surplus = surplus - extra
    return np.array(given)


def centred(own_key, extent, width, bound, pieces=(), kind=jnp.bfloat16):
    factor_of = levels(own_key, extent, pieces, -0.22, 0.18) if pieces else 1.0
    values = jax.random.normal(own_key, extent, jnp.float32) * width * factor_of
    return jnp.minimum(jnp.maximum(values, -bound), bound).astype(kind)


def setup_inputs(seed: int = 0) -> dict:
    arg_keys = jax.random.split(jax.random.key(seed), 15)
    residual = centred(arg_keys[0], (TOKENS, D), 1.0, 6.0, ((0, 128),))
    query_proj = draw_query_proj(jax.random.fold_in(arg_keys[14], 71), 0)
    key_proj = draw_key_proj(jax.random.fold_in(arg_keys[14], 71), 0)
    value_proj = centred(arg_keys[3], (TOKENS, KV_HEADS * HEAD), 1.0, 6.0, ((0, 32), (1, 4)))
    query_gain = draw_query_gain(jax.random.fold_in(arg_keys[14], 71), 0)
    key_gain = draw_key_gain(jax.random.fold_in(arg_keys[14], 71), 0)
    document_ids = jnp.searchsorted(jnp.cumsum(uneven(arg_keys[6], DOCS, TOKENS, DOC_MOST, 2)), jnp.arange(TOKENS), side="right").astype(jnp.int32)
    output_weight = centred(arg_keys[7], (HEADS * HEAD, D), (HEADS * HEAD) ** -0.5, 0.125)
    norm_gain = jnp.clip(1.0 + 0.18 * jax.random.normal(arg_keys[8], (D,), jnp.float32), 0.1, 1.9)
    expert_ids_keys = jax.random.split(jax.random.fold_in(arg_keys[9], 1), TOKENS // EROWS)
    expert_ids_turns = jax.random.permutation(jax.random.fold_in(arg_keys[9], 3), TOKENS // EROWS)
    expert_ids = jax.vmap(lambda own, number: assign_block(jax.random.fold_in(arg_keys[9], 2), own, number, EROWS, EXPERTS, TOPK, CAP, 2))(expert_ids_keys, expert_ids_turns).reshape((TOKENS, TOPK))
    route_weights = jnp.clip(0.2 + 0.8 * jax.random.uniform(arg_keys[10], (TOKENS, TOPK), jnp.float32) ** levels(arg_keys[10], (TOKENS, TOPK), ((0, 128),), -0.2, 0.2), 0.2, 1.0)
    gate_weight = centred(arg_keys[11], (EXPERTS, D, FFE), D ** -0.5, 0.125, ((0, 128),))
    up_weight = centred(arg_keys[12], (EXPERTS, D, FFE), D ** -0.5, 0.125, ((0, 128),))
    down_weight = centred(arg_keys[13], (EXPERTS, FFE, D), FFE ** -0.5, 0.25, ((0, 128),))
    return dict(residual=residual, query_proj=query_proj, key_proj=key_proj, value_proj=value_proj, query_gain=query_gain, key_gain=key_gain, document_ids=document_ids, output_weight=output_weight, norm_gain=norm_gain, expert_ids=expert_ids, route_weights=route_weights, gate_weight=gate_weight, up_weight=up_weight, down_weight=down_weight)


norm_eps = 1e-06
rope_base = 10000.0

def rotary_tables(first_row, length):
    freq_count = HEAD // 4
    inverse = 1.0 / rope_base ** (jnp.arange(freq_count, dtype=jnp.float32) / freq_count)
    position = first_row + jnp.arange(length, dtype=jnp.int32)
    grid_row = (position // GRID_W).astype(jnp.float32)
    grid_col = (position % GRID_W).astype(jnp.float32)
    angles = jnp.concatenate([grid_row[:, None] * inverse[None, :], grid_col[:, None] * inverse[None, :]], axis=1)
    return (jnp.cos(angles), jnp.sin(angles))

def norm_rotate(projected, gains, cosine, sine_table):
    length = projected.shape[0]
    values_wide = projected.astype(jnp.float32).reshape(length, -1, HEAD)
    scaled = values_wide * lax.rsqrt(lax.optimization_barrier(jnp.mean(values_wide * values_wide, axis=-1, keepdims=True)) + norm_eps) * gains
    half_size = HEAD // 2
    first_half = scaled[..., :half_size]
    second_half = scaled[..., half_size:]
    cosine_rows = cosine[:, None, :]
    sine_rows = sine_table[:, None, :]
    turned = jnp.concatenate([first_half * cosine_rows - second_half * sine_rows, first_half * sine_rows + second_half * cosine_rows], axis=-1)
    return turned.reshape(length, -1).astype(jnp.bfloat16)

def attend(query_block, key_block, value_block, query_doc, key_doc, groups):
    query_rows = query_block.shape[0]
    key_rows = key_block.shape[0]
    key_heads = key_block.shape[1] // HEAD
    query_grid = query_block.astype(jnp.float32).reshape(query_rows, key_heads, groups, HEAD)
    key_grid = key_block.astype(jnp.float32).reshape(key_rows, key_heads, HEAD)
    value_grid = value_block.astype(jnp.float32).reshape(key_rows, key_heads, HEAD)
    scores = jnp.einsum('qhgd,khd->hgqk', query_grid, key_grid) * HEAD ** (-0.5)
    same_doc = query_doc[:, None] == key_doc[None, :]
    scores = jnp.where(same_doc[None, None], scores, -jnp.inf)
    row_max = lax.optimization_barrier(jnp.max(scores, axis=-1, keepdims=True))
    weights = jnp.exp(scores - row_max)
    denominator = lax.optimization_barrier(jnp.sum(weights, axis=-1))
    rounded = weights.astype(jnp.bfloat16).astype(jnp.float32)
    weighted = jnp.einsum('hgqk,khd->hgqd', rounded, value_grid) / denominator[..., None]
    return jnp.transpose(weighted, (2, 0, 1, 3)).reshape(query_rows, key_heads * groups * HEAD).astype(jnp.bfloat16)

def reference(residual, query_proj, key_proj, value_proj, query_gain, key_gain, document_ids, output_weight, norm_gain, expert_ids, route_weights, gate_weight, up_weight, down_weight):
    tokens = query_proj.shape[0]
    cosine, sine_table = rotary_tables(jnp.int32(0), tokens)
    query_norm = norm_rotate(query_proj, query_gain, cosine, sine_table)
    key_norm = norm_rotate(key_proj, key_gain, cosine, sine_table)
    groups = HEADS // KV_HEADS
    window = min(tokens, TOK_DEV + 2 * REACH * TOK_DEV)

    def one_block(block_index):
        first_row = block_index * TOK_DEV
        key_first = jnp.clip(first_row - REACH * TOK_DEV, 0, tokens - window).astype(jnp.int32)
        query_block = lax.dynamic_slice_in_dim(query_norm, first_row, TOK_DEV, 0)
        query_doc = lax.dynamic_slice_in_dim(document_ids, first_row, TOK_DEV, 0)
        key_block = lax.dynamic_slice_in_dim(key_norm, key_first, window, 0)
        value_block = lax.dynamic_slice_in_dim(value_proj, key_first, window, 0)
        key_doc = lax.dynamic_slice_in_dim(document_ids, key_first, window, 0)
        return attend(query_block, key_block, value_block, query_doc, key_doc, groups)
    attn = lax.map(one_block, jnp.arange(tokens // TOK_DEV, dtype=jnp.int32)).reshape(tokens, HEADS * HEAD)
    hidden = (residual.astype(jnp.float32) + jnp.dot(attn, output_weight, preferred_element_type=jnp.float32)).astype(jnp.bfloat16)
    hidden_wide = hidden.astype(jnp.float32)
    normed = (hidden_wide * lax.rsqrt(lax.optimization_barrier(jnp.mean(hidden_wide * hidden_wide, axis=-1, keepdims=True)) + norm_eps) * norm_gain).astype(jnp.bfloat16)
    flat_ids = expert_ids.reshape(-1)
    flat_weights = route_weights.reshape(-1)
    top_count = expert_ids.shape[1]
    limit = N_SP * N_TP * CAP
    slot_numbers = jnp.arange(limit, dtype=jnp.int32)

    def add_expert(expert_index, running):
        matches = flat_ids == expert_index
        count = jnp.sum(matches.astype(jnp.int32))
        picked = jnp.nonzero(matches, size=limit, fill_value=0)[0].astype(jnp.int32)
        valid = (slot_numbers < count).astype(jnp.float32)
        token_index = picked // top_count
        chosen = normed[token_index]
        gate_part = jnp.dot(chosen, gate_weight[expert_index], preferred_element_type=jnp.float32)
        up_part = jnp.dot(chosen, up_weight[expert_index], preferred_element_type=jnp.float32)
        activity = (jax.nn.silu(gate_part) * up_part).astype(jnp.bfloat16)
        expert_out = jnp.dot(activity, down_weight[expert_index], preferred_element_type=jnp.float32).astype(jnp.bfloat16)
        factor = (flat_weights[picked] * valid)[:, None]
        return running.at[token_index].add(factor * expert_out.astype(jnp.float32))
    combined = lax.fori_loop(0, EXPERTS, add_expert, jnp.zeros((tokens, D), jnp.float32))
    return (hidden_wide + combined).astype(jnp.bfloat16)
```

```python
import functools

import jax
import jax.numpy as jnp
from jax import lax
from jax.experimental import pallas as pl
from jax.experimental.pallas import tpu as pltpu
from jax.sharding import PartitionSpec as P

HEAD = 128
HALF = HEAD // 2
GRID_W = 64
norm_eps = 1e-06
rope_base = 10000.0
LOW = -1e30
KB = 256
DOC_ROWS = 16
VMEM = pltpu.VMEM


def rotary_tables(first_row, length):
    count = HEAD // 4
    inverse = 1.0 / rope_base ** (jnp.arange(count, dtype=jnp.float32) / count)
    rows = (first_row // GRID_W + jnp.arange(length // GRID_W, dtype=jnp.int32)).astype(jnp.float32)
    cols = jnp.arange(GRID_W, dtype=jnp.int32).astype(jnp.float32)
    row_angle = rows[:, None] * inverse[None, :]
    col_angle = cols[:, None] * inverse[None, :]
    rz = jnp.zeros_like(row_angle)
    cz = jnp.zeros_like(col_angle)
    rc, rs = jnp.cos(row_angle), jnp.sin(row_angle)
    cc, cs = jnp.cos(col_angle), jnp.sin(col_angle)
    row_tab = jnp.stack(
        [jnp.concatenate([rc, rz, rc, rz], 1), jnp.concatenate([-rs, rz, rs, rz], 1)]
    )
    col_tab = jnp.stack(
        [jnp.concatenate([cz, cc, cz, cc], 1), jnp.concatenate([cz, -cs, cz, cs], 1)]
    )
    return row_tab, col_tab


def norm_rotate(x, gain, cos_full, sin_full):
    wide = x.astype(jnp.float32)
    mean = jnp.mean(wide * wide, axis=-1, keepdims=True)
    scaled = wide * lax.rsqrt(mean + norm_eps) * gain
    return (scaled * cos_full + pltpu.roll(scaled, HALF, 1) * sin_full).astype(jnp.bfloat16)


def key_kernel(k_ref, v_ref, doc_ref, gain_ref, row_ref, col_ref, out_ref):
    rows = k_ref.shape[0]
    gain = gain_ref[...]
    for g in range(rows // GRID_W):
        span = slice(g * GRID_W, (g + 1) * GRID_W)
        cos_full = col_ref[0] + row_ref[0, g : g + 1, :]
        sin_full = col_ref[1] + row_ref[1, g : g + 1, :]
        out_ref[span, :] = norm_rotate(k_ref[span, :], gain, cos_full, sin_full)
    out_ref[rows : 2 * rows, :] = v_ref[...]
    out_ref[2 * rows :, :] = doc_ref[...]


def query_kernel(q_ref, gain_ref, row_ref, col_ref, out_ref):
    rows, width = q_ref.shape
    gain = gain_ref[...]
    for g in range(rows // GRID_W):
        span = slice(g * GRID_W, (g + 1) * GRID_W)
        cos_full = col_ref[0] + row_ref[0, g : g + 1, :]
        sin_full = col_ref[1] + row_ref[1, g : g + 1, :]
        for h in range(width // HEAD):
            lanes = slice(h * HEAD, (h + 1) * HEAD)
            out_ref[span, lanes] = norm_rotate(q_ref[span, lanes], gain, cos_full, sin_full)


def attention_kernel(
    par_ref, edge_ref, q_ref, qdoc_ref, own, near, b1, b2, b3, b4, far, out_ref,
    k_scr, v_scr, d_scr, s_scr, mx_scr, l_scr, acc_scr,
):
    rows, width = q_ref.shape
    heads = width // HEAD
    par = par_ref[0]
    doc_rows = rows // HEAD
    slots = [
        (own, 3 + par), (near, 4 - par), (b1, 1 + par), (b2, 2 - par),
        (b3, 5 + par), (b4, 6 - par), (far, 7 * par),
    ]
    for src, slot in slots:
        at = pl.multiple_of(slot * rows, rows)
        k_scr[pl.ds(at, rows), :] = src[0:rows, :]
        v_scr[pl.ds(at, rows), :] = src[rows : 2 * rows, :]
        d_scr[slot] = src[2 * rows : 2 * rows + DOC_ROWS, :].astype(jnp.float32)
    d_scr[7 - 7 * par] = jnp.full((DOC_ROWS, HEAD), -1.0, jnp.float32)
    docs = d_scr[...]
    place = (
        lax.broadcasted_iota(jnp.int32, docs.shape, 0) * rows
        + lax.broadcasted_iota(jnp.int32, docs.shape, 1) * HEAD
        + lax.broadcasted_iota(jnp.int32, docs.shape, 2)
    )
    real = lax.broadcasted_iota(jnp.int32, docs.shape, 1) < doc_rows
    scale = HEAD ** (-0.5) * 1.4426950408889634
    block = rows // 4
    lanes = KB // HEAD
    per_slot = rows // KB
    for qs in range(4):
        first_doc = edge_ref[2 * qs]
        last_doc = edge_ref[2 * qs + 1]
        low = jnp.min(jnp.where((docs == first_doc) & real, place, 8 * rows))
        high = jnp.max(jnp.where((docs == last_doc) & real, place, -1))
        j0 = low // KB
        j1 = high // KB + 1
        span = slice(qs * block, (qs + 1) * block)
        q4 = jnp.concatenate([q_ref[span, h * HEAD : (h + 1) * HEAD] for h in range(heads)], 0)
        qdoc = qdoc_ref[span, :]
        mx_scr[...] = jnp.full(mx_scr.shape, LOW, jnp.float32)

        def scores(j, carry):
            at = pl.multiple_of(j * KB, KB)
            s = lax.dot_general(
                q4, k_scr[pl.ds(at, KB), :], (((1,), (1,)), ((), ())),
                preferred_element_type=jnp.float32,
            )
            slot = j // per_slot
            sub = (j % per_slot) * lanes
            keep = [qdoc == d_scr[slot, pl.ds(sub + t, 1), :] for t in range(lanes)]
            for h in range(heads):
                band = slice(h * block, (h + 1) * block)
                top = mx_scr[band, :]
                for t in range(lanes):
                    part = jnp.where(keep[t], s[band, t * HEAD : (t + 1) * HEAD], LOW)
                    s_scr[j, band, t * HEAD : (t + 1) * HEAD] = part
                    top = jnp.maximum(top, part)
                mx_scr[band, :] = top
            return carry

        lax.fori_loop(j0, j1, scores, 0)
        top = jnp.max(mx_scr[...], axis=1, keepdims=True) * scale
        mx_scr[...] = jnp.broadcast_to(top, mx_scr.shape)
        l_scr[...] = jnp.zeros(l_scr.shape, jnp.float32)
        acc_scr[...] = jnp.zeros(acc_scr.shape, jnp.float32)

        def weigh(j, carry):
            at = pl.multiple_of(j * KB, KB)
            top = mx_scr[...]
            parts = [
                jnp.exp2(s_scr[j, :, t * HEAD : (t + 1) * HEAD] * scale - top)
                for t in range(lanes)
            ]
            total = parts[0]
            for part in parts[1:]:
                total = total + part
            l_scr[...] += total
            p = jnp.concatenate([part.astype(jnp.bfloat16) for part in parts], axis=1)
            acc_scr[...] += jnp.dot(
                p, v_scr[pl.ds(at, KB), :], preferred_element_type=jnp.float32
            )
            return carry

        lax.fori_loop(j0, j1, weigh, 0)
        den = jnp.sum(l_scr[...], axis=1, keepdims=True)
        res = (acc_scr[...] / den).astype(jnp.bfloat16)
        for h in range(heads):
            out_ref[qs, :, h * HEAD : (h + 1) * HEAD] = res[h * block : (h + 1) * block, :]


def call(kernel, out_shape, name, scratch=(), smem=0, args=()):
    specs = [pl.BlockSpec(memory_space=pltpu.SMEM)] * smem
    specs += [pl.BlockSpec(memory_space=VMEM)] * (len(args) - smem)
    return pl.pallas_call(
        kernel,
        out_shape=out_shape,
        in_specs=specs,
        out_specs=jax.tree.map(lambda _: pl.BlockSpec(memory_space=VMEM), out_shape),
        scratch_shapes=list(scratch),
        name=name,
    )(*args)


def on_device(
    residual, query_proj, key_proj, value_proj, query_gain, key_gain, document_ids,
    output_weight, norm_gain, expert_ids, route_weights, gate_weight, up_weight, down_weight,
):
    bf16, f32 = jnp.bfloat16, jnp.float32
    sp = lax.axis_size("sp")
    index = lax.axis_index("sp")
    rows = query_proj.shape[0]
    row_tab, col_tab = rotary_tables(index * rows, rows)
    docs = document_ids.astype(bf16).reshape(rows // HEAD, HEAD)
    docs = jnp.pad(docs, ((0, DOC_ROWS - rows // HEAD), (0, 0)))
    packed = call(
        key_kernel,
        jax.ShapeDtypeStruct((2 * rows + DOC_ROWS, HEAD), bf16),
        "key_prep",
        args=(key_proj, value_proj, docs, key_gain.reshape(1, HEAD), row_tab, col_tab),
    )
    swap = [(i, i ^ 1) for i in range(sp)]
    cross = [(i, (i + 1) % sp) if i % 2 else (i, (i - 1) % sp) for i in range(sp)]
    right = [(i, (i + 2) % sp) for i in range(sp)]
    left = [(i, (i - 2) % sp) for i in range(sp)]
    par = index % 2
    from_left = lax.ppermute(packed, "sp", right)
    from_right = lax.ppermute(packed, "sp", left)
    near = lax.ppermute(packed, "sp", swap)
    far = lax.ppermute(jnp.where(par == 1, from_left, from_right), "sp", cross)
    left_pair = lax.ppermute(from_left, "sp", swap)
    right_pair = lax.ppermute(from_right, "sp", swap)

    query_norm = call(
        query_kernel,
        jax.ShapeDtypeStruct(query_proj.shape, bf16),
        "query_prep",
        args=(query_proj, query_gain.reshape(1, HEAD), row_tab, col_tab),
    )
    doc_f = document_ids.astype(f32)
    query_doc = jnp.broadcast_to(doc_f[:, None], (rows, HEAD))
    quarter = rows // 4
    edges = doc_f.reshape(4, quarter)[:, :: quarter - 1].reshape(8)
    width = query_proj.shape[1]
    attn = call(
        attention_kernel,
        jax.ShapeDtypeStruct((4, quarter, width), bf16),
        "attention",
        scratch=(
            VMEM((8 * rows, HEAD), bf16),
            VMEM((8 * rows, HEAD), bf16),
            VMEM((8, DOC_ROWS, HEAD), f32),
            VMEM((8 * rows // KB, rows, KB), f32),
            VMEM((rows, HEAD), f32),
            VMEM((rows, HEAD), f32),
            VMEM((rows, HEAD), f32),
        ),
        smem=2,
        args=(
            par.reshape(1).astype(jnp.int32), edges, query_norm, query_doc, packed, near,
            from_left, left_pair, from_right, right_pair, far,
        ),
    )
    token_rows = residual.shape[0]
    attn = attn.reshape(rows, width)
    all_heads = lax.all_to_all(attn, "tp", split_axis=0, concat_axis=1, tiled=True)
    projected = jnp.dot(all_heads, output_weight, preferred_element_type=f32)
    hidden = (residual.astype(f32) + projected).astype(bf16)
    hidden_wide = hidden.astype(f32)
    normed = (
        hidden_wide
        * lax.rsqrt(jnp.mean(hidden_wide * hidden_wide, axis=-1, keepdims=True) + norm_eps)
        * norm_gain
    ).astype(bf16)
    top_count = expert_ids.shape[1]
    experts_all = sp * lax.axis_size("tp")
    capacity = max(2, 2 * token_rows * top_count // experts_all)
    flat_ids = expert_ids.reshape(-1)
    onehot = (flat_ids[:, None] == jnp.arange(experts_all, dtype=jnp.int32)[None, :]).astype(
        jnp.int32
    )
    arrival = jnp.sum(jnp.cumsum(onehot, axis=0) * onehot, axis=1) - 1
    slot_grid = (flat_ids * capacity + arrival).reshape(token_rows, top_count)
    slots = experts_all * capacity
    hits = (
        jnp.arange(slots, dtype=jnp.int32)[:, None, None] == slot_grid[None]
    )
    placing = jnp.any(hits, axis=2).astype(bf16)
    gather = jnp.sum(jnp.where(hits, route_weights[None], 0.0), axis=2)
    gather_hi = gather.astype(bf16)
    gather_lo = (gather - gather_hi.astype(f32)).astype(bf16)
    outgoing = jnp.dot(placing, normed, preferred_element_type=f32).astype(bf16)
    outgoing = outgoing.reshape(experts_all, capacity, normed.shape[1])
    arrived = lax.all_to_all(outgoing, ("sp", "tp"), split_axis=0, concat_axis=0, tiled=True)
    sources, per, wide = arrived.shape
    flat_rows = arrived.reshape(sources * per, wide)
    gate_part = jnp.dot(flat_rows, gate_weight[0], preferred_element_type=f32)
    up_part = jnp.dot(flat_rows, up_weight[0], preferred_element_type=f32)
    activity = (jax.nn.silu(gate_part) * up_part).astype(bf16)
    expert_out = jnp.dot(activity, down_weight[0], preferred_element_type=f32).astype(bf16)
    returned = lax.all_to_all(
        expert_out.reshape(sources, per, wide), ("sp", "tp"), split_axis=0, concat_axis=0,
        tiled=True,
    ).reshape(slots, wide)
    dims = (((0,), (0,)), ((), ()))
    combined = lax.dot_general(gather_hi, returned, dims, preferred_element_type=f32)
    combined += lax.dot_general(gather_lo, returned, dims, preferred_element_type=f32)
    return (hidden_wide + combined).astype(bf16)


def solution(mesh):
    both = P(("sp", "tp"), None)
    in_specs = (
        both, P("sp", "tp"), P("sp", "tp"), P("sp", "tp"), P(), P(), P("sp"), P(), P(),
        both, both,
        P(("sp", "tp"), None, None), P(("sp", "tp"), None, None), P(("sp", "tp"), None, None),
    )
    return jax.shard_map(
        on_device, mesh=mesh, in_specs=in_specs, out_specs=both, check_vma=False
    )
```

```python
import functools

import jax
import jax.numpy as jnp
from jax import lax
from jax.experimental import pallas as pl
from jax.experimental.pallas import tpu as pltpu
from jax.sharding import PartitionSpec as P

HEAD = 128
HALF = HEAD // 2
GRID_W = 64
norm_eps = 1e-06
rope_base = 10000.0
LOW = -1e30
KB = 256
DOC_ROWS = 16
VMEM = pltpu.VMEM


def rotary_tables(first_row, length):
    count = HEAD // 4
    inverse = 1.0 / rope_base ** (jnp.arange(count, dtype=jnp.float32) / count)
    rows = (first_row // GRID_W + jnp.arange(length // GRID_W, dtype=jnp.int32)).astype(jnp.float32)
    cols = jnp.arange(GRID_W, dtype=jnp.int32).astype(jnp.float32)
    row_angle = rows[:, None] * inverse[None, :]
    col_angle = cols[:, None] * inverse[None, :]
    rz = jnp.zeros_like(row_angle)
    cz = jnp.zeros_like(col_angle)
    rc, rs = jnp.cos(row_angle), jnp.sin(row_angle)
    cc, cs = jnp.cos(col_angle), jnp.sin(col_angle)
    row_tab = jnp.stack(
        [jnp.concatenate([rc, rz, rc, rz], 1), jnp.concatenate([-rs, rz, rs, rz], 1)]
    )
    col_tab = jnp.stack(
        [jnp.concatenate([cz, cc, cz, cc], 1), jnp.concatenate([cz, -cs, cz, cs], 1)]
    )
    return row_tab, col_tab


def norm_rotate(x, gain, cos_full, sin_full):
    wide = x.astype(jnp.float32)
    mean = jnp.mean(wide * wide, axis=-1, keepdims=True)
    scaled = wide * lax.rsqrt(mean + norm_eps) * gain
    return (scaled * cos_full + pltpu.roll(scaled, HALF, 1) * sin_full).astype(jnp.bfloat16)


def key_kernel(k_ref, v_ref, doc_ref, gain_ref, row_ref, col_ref, out_ref):
    rows = k_ref.shape[0]
    gain = gain_ref[...]
    for g in range(rows // GRID_W):
        span = slice(g * GRID_W, (g + 1) * GRID_W)
        cos_full = col_ref[0] + row_ref[0, g : g + 1, :]
        sin_full = col_ref[1] + row_ref[1, g : g + 1, :]
        out_ref[span, :] = norm_rotate(k_ref[span, :], gain, cos_full, sin_full)
    out_ref[rows : 2 * rows, :] = v_ref[...]
    out_ref[2 * rows :, :] = doc_ref[...]


def query_kernel(q_ref, gain_ref, row_ref, col_ref, out_ref):
    rows, width = q_ref.shape
    gain = gain_ref[...]
    for g in range(rows // GRID_W):
        span = slice(g * GRID_W, (g + 1) * GRID_W)
        cos_full = col_ref[0] + row_ref[0, g : g + 1, :]
        sin_full = col_ref[1] + row_ref[1, g : g + 1, :]
        for h in range(width // HEAD):
            lanes = slice(h * HEAD, (h + 1) * HEAD)
            out_ref[span, lanes] = norm_rotate(q_ref[span, lanes], gain, cos_full, sin_full)


def attention_kernel(
    par_ref, edge_ref, q_ref, qdoc_ref, own, near, b1, b2, b3, b4, far, out_ref,
    k_scr, v_scr, d_scr, s_scr, mx_scr, l_scr, acc_scr,
):
    rows, width = q_ref.shape
    heads = width // HEAD
    par = par_ref[0]
    doc_rows = rows // HEAD
    slots = [
        (own, 3 + par), (near, 4 - par), (b1, 1 + par), (b2, 2 - par),
        (b3, 5 + par), (b4, 6 - par), (far, 7 * par),
    ]
    for src, slot in slots:
        at = pl.multiple_of(slot * rows, rows)
        k_scr[pl.ds(at, rows), :] = src[0:rows, :]
        v_scr[pl.ds(at, rows), :] = src[rows : 2 * rows, :]
        d_scr[slot] = src[2 * rows : 2 * rows + DOC_ROWS, :].astype(jnp.float32)
    d_scr[7 - 7 * par] = jnp.full((DOC_ROWS, HEAD), -1.0, jnp.float32)
    docs = d_scr[...]
    place = (
        lax.broadcasted_iota(jnp.int32, docs.shape, 0) * rows
        + lax.broadcasted_iota(jnp.int32, docs.shape, 1) * HEAD
        + lax.broadcasted_iota(jnp.int32, docs.shape, 2)
    )
    real = lax.broadcasted_iota(jnp.int32, docs.shape, 1) < doc_rows
    scale = HEAD ** (-0.5) * 1.4426950408889634
    block = rows // 4
    lanes = KB // HEAD
    per_slot = rows // KB
    for qs in range(4):
        first_doc = edge_ref[2 * qs]
        last_doc = edge_ref[2 * qs + 1]
        low = jnp.min(jnp.where((docs == first_doc) & real, place, 8 * rows))
        high = jnp.max(jnp.where((docs == last_doc) & real, place, -1))
        j0 = low // KB
        j1 = high // KB + 1
        span = slice(qs * block, (qs + 1) * block)
        q4 = jnp.concatenate([q_ref[span, h * HEAD : (h + 1) * HEAD] for h in range(heads)], 0)
        qdoc = qdoc_ref[span, :]
        mx_scr[...] = jnp.full(mx_scr.shape, LOW, jnp.float32)

        def scores(j, carry):
            at = pl.multiple_of(j * KB, KB)
            s = lax.dot_general(
                q4, k_scr[pl.ds(at, KB), :], (((1,), (1,)), ((), ())),
                preferred_element_type=jnp.float32,
            )
            slot = j // per_slot
            sub = (j % per_slot) * lanes
            keep = [qdoc == d_scr[slot, pl.ds(sub + t, 1), :] for t in range(lanes)]
            for h in range(heads):
                band = slice(h * block, (h + 1) * block)
                top = mx_scr[band, :]
                for t in range(lanes):
                    part = jnp.where(keep[t], s[band, t * HEAD : (t + 1) * HEAD], LOW)
                    s_scr[j, band, t * HEAD : (t + 1) * HEAD] = part
                    top = jnp.maximum(top, part)
                mx_scr[band, :] = top
            return carry

        lax.fori_loop(j0, j1, scores, 0)
        top = jnp.max(mx_scr[...], axis=1, keepdims=True) * scale
        mx_scr[...] = jnp.broadcast_to(top, mx_scr.shape)
        l_scr[...] = jnp.zeros(l_scr.shape, jnp.float32)
        acc_scr[...] = jnp.zeros(acc_scr.shape, jnp.float32)

        def weigh(j, carry):
            at = pl.multiple_of(j * KB, KB)
            top = mx_scr[...]
            parts = [
                jnp.exp2(s_scr[j, :, t * HEAD : (t + 1) * HEAD] * scale - top)
                for t in range(lanes)
            ]
            total = parts[0]
            for part in parts[1:]:
                total = total + part
            l_scr[...] += total
            p = jnp.concatenate([part.astype(jnp.bfloat16) for part in parts], axis=1)
            acc_scr[...] += jnp.dot(
                p, v_scr[pl.ds(at, KB), :], preferred_element_type=jnp.float32
            )
            return carry

        lax.fori_loop(j0, j1, weigh, 0)
        den = jnp.sum(l_scr[...], axis=1, keepdims=True)
        res = (acc_scr[...] / den).astype(jnp.bfloat16)
        for h in range(heads):
            out_ref[qs, :, h * HEAD : (h + 1) * HEAD] = res[h * block : (h + 1) * block, :]


def project_kernel(slot_ref, heads_ref, w_ref, res_ref, gain_ref, hid_ref, out_ref, n_scr):
    groups, rows, part = heads_ref.shape
    width = res_ref.shape[1]
    fold = width // HEAD
    acc = jnp.dot(heads_ref[0], w_ref[0:part, :], preferred_element_type=jnp.float32)
    for g in range(1, groups):
        acc += jnp.dot(
            heads_ref[g], w_ref[g * part : (g + 1) * part, :], preferred_element_type=jnp.float32
        )
    hidden = (res_ref[...].astype(jnp.float32) + acc).astype(jnp.bfloat16)
    hid_ref[...] = hidden
    wide = hidden.astype(jnp.float32)
    mean = jnp.mean(wide * wide, axis=-1, keepdims=True)
    normed = wide * lax.rsqrt(mean + norm_eps) * gain_ref[...]
    for c in range(fold):
        n_scr[pl.ds(c, rows, stride=fold), :] = normed[:, c * HEAD : (c + 1) * HEAD]
    zero = jnp.zeros((32,) + out_ref.shape[1:], jnp.bfloat16)
    for b in range(out_ref.shape[0] // 32):
        out_ref[b * 32 : (b + 1) * 32] = zero

    def place(step, carry):
        for u in range(8):
            token = step * 8 + u
            tile = n_scr[pl.ds(pl.multiple_of(token * fold, fold), fold), :].astype(jnp.bfloat16)
            out_ref[slot_ref[2 * token]] = tile
            out_ref[slot_ref[2 * token + 1]] = tile
        return carry

    lax.fori_loop(0, rows // 8, place, 0)


def expert_kernel(in_ref, gate_ref, up_ref, down_ref, out_ref, f_scr, x_scr):
    slots, fold, _ = in_ref.shape
    part = slots // 4
    for b in range(4):
        band = slice(b * part, (b + 1) * part)
        f_scr[b * part * fold : (b + 1) * part * fold, :] = (
            in_ref[band].astype(jnp.float32).reshape(part * fold, HEAD)
        )
        for c in range(fold):
            x_scr[band, c * HEAD : (c + 1) * HEAD] = f_scr[
                pl.ds(b * part * fold + c, part, stride=fold), :
            ].astype(jnp.bfloat16)
    x = x_scr[...]
    gate = jnp.dot(x, gate_ref[0], preferred_element_type=jnp.float32)
    up = jnp.dot(x, up_ref[0], preferred_element_type=jnp.float32)
    act = (jax.nn.silu(gate) * up).astype(jnp.bfloat16)
    step = 2
    for n in range(fold // step):
        y = jnp.dot(
            act, down_ref[0, :, n * step * HEAD : (n + 1) * step * HEAD],
            preferred_element_type=jnp.float32,
        )
        for t in range(step):
            f_scr[pl.ds(n * step + t, slots, stride=fold), :] = y[:, t * HEAD : (t + 1) * HEAD]
    for b in range(4):
        out_ref[b * part : (b + 1) * part] = (
            f_scr[b * part * fold : (b + 1) * part * fold, :]
            .reshape(part, fold, HEAD)
            .astype(jnp.bfloat16)
        )


def combine_kernel(slot_ref, weight_ref, ret_ref, hid_ref, out_ref, c_scr):
    rows, width = hid_ref.shape
    fold = width // HEAD

    def gather(step, carry):
        for u in range(8):
            token = step * 8 + u
            one = ret_ref[slot_ref[2 * token]].astype(jnp.float32) * weight_ref[2 * token]
            two = ret_ref[slot_ref[2 * token + 1]].astype(jnp.float32) * weight_ref[2 * token + 1]
            c_scr[pl.ds(pl.multiple_of(token * fold, fold), fold), :] = one + two
        return carry

    lax.fori_loop(0, rows // 8, gather, 0)
    for c in range(fold):
        lanes = slice(c * HEAD, (c + 1) * HEAD)
        out_ref[:, lanes] = (
            hid_ref[:, lanes].astype(jnp.float32) + c_scr[pl.ds(c, rows, stride=fold), :]
        ).astype(jnp.bfloat16)


def call(kernel, out_shape, name, limit, scratch=(), smem=0, args=()):
    specs = [pl.BlockSpec(memory_space=pltpu.SMEM)] * smem
    specs += [pl.BlockSpec(memory_space=VMEM)] * (len(args) - smem)
    return pl.pallas_call(
        kernel,
        out_shape=out_shape,
        in_specs=specs,
        out_specs=jax.tree.map(lambda _: pl.BlockSpec(memory_space=VMEM), out_shape),
        scratch_shapes=list(scratch),
        name=name,
        compiler_params=pltpu.CompilerParams(vmem_limit_bytes=limit * 2**20),
    )(*args)


def on_device(
    residual, query_proj, key_proj, value_proj, query_gain, key_gain, document_ids,
    output_weight, norm_gain, expert_ids, route_weights, gate_weight, up_weight, down_weight,
):
    bf16, f32 = jnp.bfloat16, jnp.float32
    sp = lax.axis_size("sp")
    index = lax.axis_index("sp")
    rows = query_proj.shape[0]
    row_tab, col_tab = rotary_tables(index * rows, rows)
    docs = document_ids.astype(bf16).reshape(rows // HEAD, HEAD)
    docs = jnp.pad(docs, ((0, DOC_ROWS - rows // HEAD), (0, 0)))
    packed = call(
        key_kernel,
        jax.ShapeDtypeStruct((2 * rows + DOC_ROWS, HEAD), bf16),
        "key_prep", 8,
        args=(key_proj, value_proj, docs, key_gain.reshape(1, HEAD), row_tab, col_tab),
    )
    swap = [(i, i ^ 1) for i in range(sp)]
    cross = [(i, (i + 1) % sp) if i % 2 else (i, (i - 1) % sp) for i in range(sp)]
    right = [(i, (i + 2) % sp) for i in range(sp)]
    left = [(i, (i - 2) % sp) for i in range(sp)]
    par = index % 2
    from_left = lax.ppermute(packed, "sp", right)
    from_right = lax.ppermute(packed, "sp", left)
    near = lax.ppermute(packed, "sp", swap)
    far = lax.ppermute(jnp.where(par == 1, from_left, from_right), "sp", cross)
    left_pair = lax.ppermute(from_left, "sp", swap)
    right_pair = lax.ppermute(from_right, "sp", swap)

    query_norm = call(
        query_kernel,
        jax.ShapeDtypeStruct(query_proj.shape, bf16),
        "query_prep", 8,
        args=(query_proj, query_gain.reshape(1, HEAD), row_tab, col_tab),
    )
    doc_f = document_ids.astype(f32)
    query_doc = jnp.broadcast_to(doc_f[:, None], (rows, HEAD))
    quarter = rows // 4
    edges = doc_f.reshape(4, quarter)[:, :: quarter - 1].reshape(8)
    width = query_proj.shape[1]
    attn = call(
        attention_kernel,
        jax.ShapeDtypeStruct((4, quarter, width), bf16),
        "attention", 20,
        scratch=(
            VMEM((8 * rows, HEAD), bf16),
            VMEM((8 * rows, HEAD), bf16),
            VMEM((8, DOC_ROWS, HEAD), f32),
            VMEM((8 * rows // KB, rows, KB), f32),
            VMEM((rows, HEAD), f32),
            VMEM((rows, HEAD), f32),
            VMEM((rows, HEAD), f32),
        ),
        smem=2,
        args=(
            par.reshape(1).astype(jnp.int32), edges, query_norm, query_doc, packed, near,
            from_left, left_pair, from_right, right_pair, far,
        ),
    )
    token_rows, wide = residual.shape
    fold = wide // HEAD
    top_count = expert_ids.shape[1]
    experts_all = sp * lax.axis_size("tp")
    capacity = max(2, 2 * token_rows * top_count // experts_all)
    slots = experts_all * capacity
    flat_ids = expert_ids.reshape(-1)
    onehot = (flat_ids[:, None] == jnp.arange(experts_all, dtype=jnp.int32)[None, :]).astype(
        jnp.int32
    )
    arrival = jnp.sum(jnp.cumsum(onehot, axis=0) * onehot, axis=1) - 1
    slot = flat_ids * capacity + arrival
    heads = lax.all_to_all(attn, "tp", split_axis=0, concat_axis=0, tiled=True)
    hidden, outgoing = call(
        project_kernel,
        (
            jax.ShapeDtypeStruct((token_rows, wide), bf16),
            jax.ShapeDtypeStruct((slots, fold, HEAD), bf16),
        ),
        "project", 24,
        scratch=(VMEM((token_rows * fold, HEAD), f32),),
        smem=1,
        args=(slot, heads, output_weight, residual, norm_gain.reshape(1, wide)),
    )

    def exchange(x):
        x = x.reshape(experts_all, capacity * fold, HEAD)
        x = lax.all_to_all(x, ("sp", "tp"), split_axis=0, concat_axis=0, tiled=True)
        return x.reshape(slots, fold, HEAD)

    arrived = exchange(outgoing)
    expert_out = call(
        expert_kernel,
        jax.ShapeDtypeStruct((slots, fold, HEAD), bf16),
        "experts", 32,
        scratch=(VMEM((slots * fold, HEAD), f32), VMEM((slots, wide), bf16)),
        args=(arrived, gate_weight, up_weight, down_weight),
    )
    returned = exchange(expert_out)
    return call(
        combine_kernel,
        jax.ShapeDtypeStruct((token_rows, wide), bf16),
        "combine", 16,
        scratch=(VMEM((token_rows * fold, HEAD), f32),),
        smem=2,
        args=(slot, route_weights.reshape(-1), returned, hidden),
    )


def solution(mesh):
    both = P(("sp", "tp"), None)
    in_specs = (
        both, P("sp", "tp"), P("sp", "tp"), P("sp", "tp"), P(), P(), P("sp"), P(), P(),
        both, both,
        P(("sp", "tp"), None, None), P(("sp", "tp"), None, None), P(("sp", "tp"), None, None),
    )
    return jax.shard_map(
        on_device, mesh=mesh, in_specs=in_specs, out_specs=both, check_vma=False
    )
```

```python
import functools

import jax
import jax.numpy as jnp
from jax import lax
from jax.experimental import pallas as pl
from jax.experimental.pallas import tpu as pltpu
from jax.sharding import PartitionSpec as P


HEAD = 128
HALF = HEAD // 2
GRID_W = 64
norm_eps = 1e-06
rope_base = 10000.0
LOW = -1e30
KB = 512
DOC_ROWS = 16
VMEM = pltpu.VMEM


def rotary_tables(first_row, length):
    count = HEAD // 4
    inverse = 1.0 / rope_base ** (jnp.arange(count, dtype=jnp.float32) / count)
    rows = (first_row // GRID_W + jnp.arange(length // GRID_W, dtype=jnp.int32)).astype(jnp.float32)
    cols = jnp.arange(GRID_W, dtype=jnp.int32).astype(jnp.float32)
    row_angle = rows[:, None] * inverse[None, :]
    col_angle = cols[:, None] * inverse[None, :]
    rz = jnp.zeros_like(row_angle)
    cz = jnp.zeros_like(col_angle)
    rc, rs = jnp.cos(row_angle), jnp.sin(row_angle)
    cc, cs = jnp.cos(col_angle), jnp.sin(col_angle)
    row_tab = jnp.stack(
        [jnp.concatenate([rc, rz, rc, rz], 1), jnp.concatenate([-rs, rz, rs, rz], 1)]
    )
    col_tab = jnp.stack(
        [jnp.concatenate([cz, cc, cz, cc], 1), jnp.concatenate([cz, -cs, cz, cs], 1)]
    )
    return row_tab, col_tab


def norm_rotate(x, gain, cos_full, sin_full):
    wide = x.astype(jnp.float32)
    mean = jnp.mean(wide * wide, axis=-1, keepdims=True)
    scaled = wide * lax.rsqrt(mean + norm_eps) * gain
    return (scaled * cos_full + pltpu.roll(scaled, HALF, 1) * sin_full).astype(jnp.bfloat16)


def key_kernel(
    k_hbm, v_hbm, doc_hbm, gain_hbm, row_ref, col_ref, out_ref, k_ref, doc_ref, gain_ref, sems
):
    rows = k_ref.shape[0]
    copies = [
        pltpu.make_async_copy(k_hbm, k_ref, sems.at[0]),
        pltpu.make_async_copy(gain_hbm, gain_ref, sems.at[1]),
        pltpu.make_async_copy(doc_hbm, doc_ref, sems.at[2]),
        pltpu.make_async_copy(v_hbm, out_ref.at[pl.ds(rows, rows), :], sems.at[3]),
    ]
    for copy in copies:
        copy.start()
    for copy in copies[:3]:
        copy.wait()
    docs = doc_ref[...].astype(jnp.float32).astype(jnp.bfloat16)
    pad = jnp.zeros((DOC_ROWS - docs.shape[0], HEAD), jnp.bfloat16)
    out_ref[2 * rows :, :] = jnp.concatenate([docs, pad], 0)
    gain = gain_ref[...]
    for g in range(rows // GRID_W):
        span = slice(g * GRID_W, (g + 1) * GRID_W)
        cos_full = col_ref[0] + row_ref[0, g : g + 1, :]
        sin_full = col_ref[1] + row_ref[1, g : g + 1, :]
        out_ref[span, :] = norm_rotate(k_ref[span, :], gain, cos_full, sin_full)
    copies[3].wait()


def query_kernel(
    q_hbm, ids_hbm, doc_hbm, gain_hbm, row_ref, col_ref, out_ref, qdoc_ref, slot_ref,
    q_ref, ids_ref, doc_ref, gain_ref, sems, *, capacity,
):
    copies = [
        pltpu.make_async_copy(src, dst, sems.at[n])
        for n, (src, dst) in enumerate(
            [(q_hbm, q_ref), (gain_hbm, gain_ref), (doc_hbm, doc_ref), (ids_hbm, ids_ref)]
        )
    ]
    for copy in copies:
        copy.start()
    for copy in copies:
        copy.wait()
    rows, width = q_ref.shape
    gain = gain_ref[...]
    for g in range(rows // GRID_W):
        span = slice(g * GRID_W, (g + 1) * GRID_W)
        cos_full = col_ref[0] + row_ref[0, g : g + 1, :]
        sin_full = col_ref[1] + row_ref[1, g : g + 1, :]
        for h in range(width // HEAD):
            lanes = slice(h * HEAD, (h + 1) * HEAD)
            out_ref[span, lanes] = norm_rotate(q_ref[span, lanes], gain, cos_full, sin_full)
    for t in range(doc_ref.shape[0]):
        line = jnp.broadcast_to(doc_ref[t : t + 1, :].astype(jnp.float32), (HEAD, HEAD))
        qdoc_ref[t * HEAD : (t + 1) * HEAD, :] = line.T
    choices, tokens = ids_ref.shape
    sub = lax.broadcasted_iota(jnp.int32, (HEAD, tokens), 0)
    lane = lax.broadcasted_iota(jnp.int32, (tokens, tokens), 1)
    upper = (lax.broadcasted_iota(jnp.int32, (tokens, tokens), 0) <= lane).astype(jnp.float32)
    upper = upper.astype(jnp.bfloat16)
    before = jnp.zeros((HEAD, 1), jnp.float32)
    for k in range(choices):
        ids = ids_ref[k : k + 1, :]
        hit = (sub == ids).astype(jnp.float32)
        running = before + jnp.dot(
            hit.astype(jnp.bfloat16), upper, preferred_element_type=jnp.float32
        )
        arrival = jnp.sum(running * hit, axis=0, keepdims=True) - 1.0
        slot_ref[k : k + 1, :] = ids * capacity + arrival.astype(jnp.int32)
        before = before + jnp.sum(hit, axis=1, keepdims=True)


def attention_kernel(
    par_ref, edge_ref, w_hbm, q_ref, qdoc_ref, own, near, b1, b2, b3, b4, far, out_ref, w_ref,
    k_scr, v_scr, d_scr, s_even, s_odd, mx_even, mx_odd, l_scr, acc_scr, sem,
):
    fetch = pltpu.make_async_copy(w_hbm, w_ref, sem)
    fetch.start()
    rows, width = q_ref.shape
    heads = width // HEAD
    par = par_ref[0]
    tiles = rows // HEAD
    slots = [
        (own, 3 + par), (near, 4 - par), (b1, 1 + par), (b2, 2 - par),
        (b3, 5 + par), (b4, 6 - par), (far, 7 * par),
    ]
    for src, slot in slots:
        at = pl.multiple_of(slot * rows, rows)
        k_scr[pl.ds(at, rows), :] = src[0:rows, :]
        v_scr[pl.ds(at, rows), :] = src[rows : 2 * rows, :]
        docs = src[2 * rows : 2 * rows + DOC_ROWS, :].astype(jnp.float32)
        for t in range(tiles):
            d_scr[slot * tiles + t] = jnp.broadcast_to(docs[t : t + 1, :], (8, HEAD))
    for slot in (7 - 7 * par, 8):
        at = pl.multiple_of(slot * rows, rows)
        k_scr[pl.ds(at, rows), :] = jnp.zeros((rows, HEAD), jnp.bfloat16)
        v_scr[pl.ds(at, rows), :] = jnp.zeros((rows, HEAD), jnp.bfloat16)
        for t in range(tiles):
            d_scr[slot * tiles + t] = jnp.full((8, HEAD), -1.0, jnp.float32)
    docs = d_scr[...]
    place = lax.broadcasted_iota(jnp.int32, docs.shape, 0) * HEAD + lax.broadcasted_iota(
        jnp.int32, docs.shape, 2
    )
    scale = HEAD ** (-0.5) * 1.4426950408889634
    block = rows // 4
    parts = KB // HEAD
    pieces = block // 16
    starts, counts = [], []
    for qs in range(4):
        first = edge_ref[qs, 0].astype(jnp.float32)
        last = edge_ref[qs, block - 1].astype(jnp.float32)
        low = jnp.min(jnp.where(docs == first, place, 8 * rows))
        high = jnp.max(jnp.where(docs == last, place, -1))
        start = (low // HEAD) * HEAD
        starts.append(start)
        counts.append((high - start) // KB + 1)
    s_refs = (s_even, s_odd)
    mx_refs = (mx_even, mx_odd)
    spare = s_even.shape[0] - 2
    for ref in s_refs:
        ref[spare] = jnp.full(ref.shape[1:], LOW, jnp.float32)

    def scores(qs, i):
        s_ref, mx_ref = s_refs[qs % 2], mx_refs[qs % 2]
        at = pl.multiple_of(jnp.minimum(starts[qs] + i * KB, 8 * rows), HEAD)
        index = jnp.where(i < counts[qs], i, spare + 1)
        base = qs * block
        q4 = jnp.concatenate(
            [
                q_ref[base + r * 16 : base + (r + 1) * 16, h * HEAD : (h + 1) * HEAD]
                for r in range(pieces)
                for h in range(heads)
            ],
            0,
        )
        s = lax.dot_general(
            q4, k_scr[pl.ds(at, KB), :], (((1,), (1,)), ((), ())),
            preferred_element_type=jnp.float32,
        )
        tile = at // HEAD
        key_docs = [d_scr[tile + t] for t in range(parts)]
        key_docs = [jnp.concatenate([d, d], 0) for d in key_docs]
        for r in range(pieces):
            qdoc = qdoc_ref[base + r * 16 : base + (r + 1) * 16, :]
            keep = [qdoc == d for d in key_docs]
            for h in range(heads):
                band = slice((r * heads + h) * 16, (r * heads + h + 1) * 16)
                top = mx_ref[band, :]
                for t in range(parts):
                    lanes = slice(t * HEAD, (t + 1) * HEAD)
                    part = jnp.where(keep[t], s[band, lanes], LOW)
                    s_ref[index, band, lanes] = part
                    top = jnp.maximum(top, part)
                mx_ref[band, :] = top

    def weigh(qs, i):
        s_ref, mx_ref = s_refs[qs % 2], mx_refs[qs % 2]
        at = pl.multiple_of(jnp.minimum(starts[qs] + i * KB, 8 * rows), HEAD)
        index = jnp.where(i < counts[qs], i, spare)
        top = mx_ref[...]
        probs = []
        total = l_scr[...]
        for t in range(parts):
            e = jnp.exp2(s_ref[index, :, t * HEAD : (t + 1) * HEAD] * scale - top)
            total = total + e
            probs.append(e.astype(jnp.bfloat16))
        l_scr[...] = total
        acc_scr[...] += jnp.dot(
            jnp.concatenate(probs, axis=1), v_scr[pl.ds(at, KB), :],
            preferred_element_type=jnp.float32,
        )

    for step in range(5):
        trip = counts[step] if step == 0 else counts[step - 1]
        if 0 < step < 4:
            trip = jnp.maximum(trip, counts[step])
        if step < 4:
            mx_refs[step % 2][...] = jnp.full(mx_even.shape, LOW, jnp.float32)
        if step > 0:
            l_scr[...] = jnp.zeros(l_scr.shape, jnp.float32)
            acc_scr[...] = jnp.zeros(acc_scr.shape, jnp.float32)

        def body(i, carry, step=step):
            if step > 0:
                weigh(step - 1, i)
            if step < 4:
                scores(step, i)
            return carry

        lax.fori_loop(0, trip, body, 0)
        if step < 4:
            ref = mx_refs[step % 2]
            ref[...] = jnp.broadcast_to(
                jnp.max(ref[...], axis=1, keepdims=True) * scale, ref.shape
            )
        if step > 0:
            den = jnp.sum(l_scr[...], axis=1, keepdims=True)
            res = (acc_scr[...] / den).astype(jnp.bfloat16)
            for r in range(pieces):
                for h in range(heads):
                    at = (r * heads + h) * 16
                    out_ref[step - 1, r * 16 : (r + 1) * 16, h * HEAD : (h + 1) * HEAD] = res[
                        at : at + 16, :
                    ]
    fetch.wait()


def project_kernel(slot_ref, heads_ref, w_ref, res_ref, gain_ref, hid_ref, out_ref, n_scr):
    groups, rows, part = heads_ref.shape
    width = res_ref.shape[1]
    fold = width // HEAD
    acc = jnp.dot(heads_ref[0], w_ref[0:part, :], preferred_element_type=jnp.float32)
    for g in range(1, groups):
        acc += jnp.dot(
            heads_ref[g], w_ref[g * part : (g + 1) * part, :], preferred_element_type=jnp.float32
        )
    hidden = (res_ref[...].astype(jnp.float32) + acc).astype(jnp.bfloat16)
    hid_ref[...] = hidden
    wide = hidden.astype(jnp.float32)
    mean = jnp.mean(wide * wide, axis=-1, keepdims=True)
    normed = wide * lax.rsqrt(mean + norm_eps) * gain_ref[...]
    for c in range(fold):
        n_scr[pl.ds(c, rows, stride=fold), :] = normed[:, c * HEAD : (c + 1) * HEAD]
    zero = jnp.zeros((32,) + out_ref.shape[1:], jnp.bfloat16)
    for b in range(out_ref.shape[0] // 32):
        out_ref[b * 32 : (b + 1) * 32] = zero

    def place(step, carry):
        for u in range(8):
            token = step * 8 + u
            tile = n_scr[pl.ds(pl.multiple_of(token * fold, fold), fold), :].astype(jnp.bfloat16)
            out_ref[slot_ref[0, token]] = tile
            out_ref[slot_ref[1, token]] = tile
        return carry

    lax.fori_loop(0, rows // 8, place, 0)


def expert_kernel(in_ref, gate_ref, up_ref, down_ref, out_ref, f_scr, x_scr):
    slots, fold, _ = in_ref.shape
    part = slots // 4
    for b in range(4):
        band = slice(b * part, (b + 1) * part)
        f_scr[b * part * fold : (b + 1) * part * fold, :] = (
            in_ref[band].astype(jnp.float32).reshape(part * fold, HEAD)
        )
        for c in range(fold):
            x_scr[band, c * HEAD : (c + 1) * HEAD] = f_scr[
                pl.ds(b * part * fold + c, part, stride=fold), :
            ].astype(jnp.bfloat16)
    x = x_scr[...]
    gate = jnp.dot(x, gate_ref[0], preferred_element_type=jnp.float32)
    up = jnp.dot(x, up_ref[0], preferred_element_type=jnp.float32)
    act = (jax.nn.silu(gate) * up).astype(jnp.bfloat16)
    step = 2
    for n in range(fold // step):
        y = jnp.dot(
            act, down_ref[0, :, n * step * HEAD : (n + 1) * step * HEAD],
            preferred_element_type=jnp.float32,
        )
        for t in range(step):
            f_scr[pl.ds(n * step + t, slots, stride=fold), :] = y[:, t * HEAD : (t + 1) * HEAD]
    for b in range(4):
        out_ref[b * part : (b + 1) * part] = (
            f_scr[b * part * fold : (b + 1) * part * fold, :]
            .reshape(part, fold, HEAD)
            .astype(jnp.bfloat16)
        )


def combine_kernel(slot_ref, weight_ref, ret_ref, hid_ref, out_ref, c_scr):
    rows, width = hid_ref.shape
    fold = width // HEAD

    def gather(step, carry):
        for u in range(8):
            token = step * 8 + u
            one = ret_ref[slot_ref[0, token]].astype(jnp.float32) * weight_ref[0, token]
            two = ret_ref[slot_ref[1, token]].astype(jnp.float32) * weight_ref[1, token]
            c_scr[pl.ds(pl.multiple_of(token * fold, fold), fold), :] = one + two
        return carry

    lax.fori_loop(0, rows // 8, gather, 0)
    for c in range(fold):
        lanes = slice(c * HEAD, (c + 1) * HEAD)
        out_ref[:, lanes] = (
            hid_ref[:, lanes].astype(jnp.float32) + c_scr[pl.ds(c, rows, stride=fold), :]
        ).astype(jnp.bfloat16)


def in_hbm(x):
    return pltpu.with_memory_space_constraint(x, pltpu.HBM)


def call(kernel, out_shape, limit, scratch=(), smem=0, args=(), hbm=0):
    specs = [pl.BlockSpec(memory_space=pltpu.SMEM)] * smem
    specs += [pl.BlockSpec(memory_space=pltpu.HBM)] * hbm
    specs += [pl.BlockSpec(memory_space=VMEM)] * (len(args) - smem - hbm)
    return pl.pallas_call(
        kernel,
        out_shape=out_shape,
        in_specs=specs,
        out_specs=jax.tree.map(lambda _: pl.BlockSpec(memory_space=VMEM), out_shape),
        scratch_shapes=list(scratch),
        compiler_params=pltpu.CompilerParams(vmem_limit_bytes=limit * 2**20),
    )(*args)


def on_device(
    residual, query_proj, key_proj, value_proj, query_gain, key_gain, document_ids,
    output_weight, norm_gain, expert_ids, route_weights, gate_weight, up_weight, down_weight,
):
    bf16, f32 = jnp.bfloat16, jnp.float32
    sp = lax.axis_size("sp")
    index = lax.axis_index("sp")
    rows = query_proj.shape[0]
    row_tab, col_tab = rotary_tables(index * rows, rows)
    doc_lines = document_ids.reshape(rows // HEAD, HEAD)
    packed = pl.pallas_call(
        key_kernel,
        out_shape=jax.ShapeDtypeStruct((2 * rows + DOC_ROWS, HEAD), bf16),
        in_specs=[pl.BlockSpec(memory_space=pltpu.HBM)] * 4
        + [pl.BlockSpec(memory_space=VMEM)] * 2,
        out_specs=pl.BlockSpec(memory_space=VMEM),
        scratch_shapes=[
            VMEM((rows, HEAD), bf16),
            VMEM((rows // HEAD, HEAD), jnp.int32),
            VMEM((1, HEAD), f32),
            pltpu.SemaphoreType.DMA((4,)),
        ],
        name="key_prep",
        compiler_params=pltpu.CompilerParams(vmem_limit_bytes=8 * 2**20),
    )(
        in_hbm(key_proj), in_hbm(value_proj), in_hbm(doc_lines),
        in_hbm(key_gain.reshape(1, HEAD)), row_tab, col_tab,
    )
    swap = [(i, i ^ 1) for i in range(sp)]
    cross = [(i, (i + 1) % sp) if i % 2 else (i, (i - 1) % sp) for i in range(sp)]
    right = [(i, (i + 2) % sp) for i in range(sp)]
    left = [(i, (i - 2) % sp) for i in range(sp)]
    par = index % 2
    from_left = lax.ppermute(packed, "sp", right)
    from_right = lax.ppermute(packed, "sp", left)
    near = lax.ppermute(packed, "sp", swap)
    far = lax.ppermute(jnp.where(par == 1, from_left, from_right), "sp", cross)
    left_pair = lax.ppermute(from_left, "sp", swap)
    right_pair = lax.ppermute(from_right, "sp", swap)

    quarter = rows // 4
    width = query_proj.shape[1]
    token_rows, wide = residual.shape
    fold = wide // HEAD
    top_count = expert_ids.shape[1]
    experts_all = sp * lax.axis_size("tp")
    capacity = max(2, 2 * token_rows * top_count // experts_all)
    slots = experts_all * capacity
    query_norm, query_doc, slot = call(
        functools.partial(query_kernel, capacity=capacity),
        (
            jax.ShapeDtypeStruct(query_proj.shape, bf16),
            jax.ShapeDtypeStruct((rows, HEAD), f32),
            jax.ShapeDtypeStruct((top_count, token_rows), jnp.int32),
        ),
        8,
        scratch=(
            VMEM(query_proj.shape, bf16),
            VMEM((top_count, token_rows), jnp.int32),
            VMEM(doc_lines.shape, jnp.int32),
            VMEM((1, HEAD), f32),
            pltpu.SemaphoreType.DMA((4,)),
        ),
        hbm=4,
        args=(
            in_hbm(query_proj), in_hbm(expert_ids.T), in_hbm(doc_lines),
            in_hbm(query_gain.reshape(1, HEAD)), row_tab, col_tab,
        ),
    )
    anywhere = pl.BlockSpec(memory_space=pltpu.HBM)
    smem = pl.BlockSpec(memory_space=pltpu.SMEM)
    vmem = pl.BlockSpec(memory_space=VMEM)
    attn, weight_near = pl.pallas_call(
        attention_kernel,
        out_shape=(
            jax.ShapeDtypeStruct((4, quarter, width), bf16),
            jax.ShapeDtypeStruct(output_weight.shape, bf16),
        ),
        in_specs=[smem, smem, anywhere] + [vmem] * 9,
        out_specs=(vmem, vmem),
        scratch_shapes=[
            VMEM((9 * rows, HEAD), bf16),
            VMEM((9 * rows, HEAD), bf16),
            VMEM((9 * rows // HEAD, 8, HEAD), f32),
            VMEM((10, rows, KB), f32),
            VMEM((10, rows, KB), f32),
            VMEM((rows, HEAD), f32),
            VMEM((rows, HEAD), f32),
            VMEM((rows, HEAD), f32),
            VMEM((rows, HEAD), f32),
            pltpu.SemaphoreType.DMA,
        ],
        name="attention",
        compiler_params=pltpu.CompilerParams(vmem_limit_bytes=40 * 2**20),
    )(
        par.reshape(1).astype(jnp.int32), doc_lines, in_hbm(output_weight), query_norm, query_doc, packed,
        near, from_left, left_pair, from_right, right_pair, far,
    )
    heads = lax.all_to_all(attn, "tp", split_axis=0, concat_axis=0, tiled=True)
    hidden, outgoing = call(
        project_kernel,
        (
            jax.ShapeDtypeStruct((token_rows, wide), bf16),
            jax.ShapeDtypeStruct((slots, fold, HEAD), bf16),
        ),
        24,
        scratch=(VMEM((token_rows * fold, HEAD), f32),),
        smem=1,
        args=(slot, heads, weight_near, residual, norm_gain.reshape(1, wide)),
    )

    def exchange(x):
        x = x.reshape(experts_all, capacity * fold, HEAD)
        x = lax.all_to_all(x, ("sp", "tp"), split_axis=0, concat_axis=0, tiled=True)
        return x.reshape(slots, fold, HEAD)

    arrived = exchange(outgoing)
    expert_out = call(
        expert_kernel,
        jax.ShapeDtypeStruct((slots, fold, HEAD), bf16),
        32,
        scratch=(VMEM((slots * fold, HEAD), f32), VMEM((slots, wide), bf16)),
        args=(arrived, gate_weight, up_weight, down_weight),
    )
    returned = exchange(expert_out)
    return call(
        combine_kernel,
        jax.ShapeDtypeStruct((token_rows, wide), bf16),
        16,
        scratch=(VMEM((token_rows * fold, HEAD), f32),),
        smem=2,
        args=(slot, route_weights.T, returned, hidden),
    )


def solution(mesh):
    both = P(("sp", "tp"), None)
    in_specs = (
        both, P("sp", "tp"), P("sp", "tp"), P("sp", "tp"), P(), P(), P("sp"), P(), P(),
        both, both,
        P(("sp", "tp"), None, None), P(("sp", "tp"), None, None), P(("sp", "tp"), None, None),
    )

    return jax.shard_map(on_device, mesh=mesh, in_specs=in_specs, out_specs=both, check_vma=False)
```

```python
import functools

import jax
import jax.numpy as jnp
from jax import lax
from jax.experimental import pallas as pl
from jax.experimental.pallas import tpu as pltpu
from jax.sharding import PartitionSpec as P


HEAD = 128
HALF = HEAD // 2
GRID_W = 64
norm_eps = 1e-06
rope_base = 10000.0
LOW = -1e30
DOC_ROWS = 16
VMEM = pltpu.VMEM


def rotary_tables(first_row, length):
    count = HEAD // 4
    inverse = 1.0 / rope_base ** (jnp.arange(count, dtype=jnp.float32) / count)
    rows = (first_row // GRID_W + jnp.arange(length // GRID_W, dtype=jnp.int32)).astype(jnp.float32)
    cols = jnp.arange(GRID_W, dtype=jnp.int32).astype(jnp.float32)
    row_angle = rows[:, None] * inverse[None, :]
    col_angle = cols[:, None] * inverse[None, :]
    rz = jnp.zeros_like(row_angle)
    cz = jnp.zeros_like(col_angle)
    rc, rs = jnp.cos(row_angle), jnp.sin(row_angle)
    cc, cs = jnp.cos(col_angle), jnp.sin(col_angle)
    row_tab = jnp.stack(
        [jnp.concatenate([rc, rz, rc, rz], 1), jnp.concatenate([-rs, rz, rs, rz], 1)]
    )
    col_tab = jnp.stack(
        [jnp.concatenate([cz, cc, cz, cc], 1), jnp.concatenate([cz, -cs, cz, cs], 1)]
    )
    return row_tab, col_tab


def norm_rotate(x, gain, cos_full, sin_full):
    wide = x.astype(jnp.float32)
    mean = jnp.mean(wide * wide, axis=-1, keepdims=True)
    scaled = wide * lax.rsqrt(mean + norm_eps) * gain
    return (scaled * cos_full + pltpu.roll(scaled, HALF, 1) * sin_full).astype(jnp.bfloat16)


def key_kernel(
    k_hbm, v_hbm, doc_hbm, gain_hbm, row_ref, col_ref, out_ref, k_ref, doc_ref, gain_ref, sems
):
    rows = k_ref.shape[0]
    copies = [
        pltpu.make_async_copy(k_hbm, k_ref, sems.at[0]),
        pltpu.make_async_copy(gain_hbm, gain_ref, sems.at[1]),
        pltpu.make_async_copy(doc_hbm, doc_ref, sems.at[2]),
        pltpu.make_async_copy(v_hbm, out_ref.at[pl.ds(rows, rows), :], sems.at[3]),
    ]
    for copy in copies:
        copy.start()
    for copy in copies[:3]:
        copy.wait()
    docs = (doc_ref[...].astype(jnp.float32) + 1.0).astype(jnp.bfloat16)
    pad = jnp.zeros((DOC_ROWS - docs.shape[0], HEAD), jnp.bfloat16)
    out_ref[2 * rows :, :] = jnp.concatenate([docs, pad], 0)
    gain = gain_ref[...]
    for g in range(rows // GRID_W):
        span = slice(g * GRID_W, (g + 1) * GRID_W)
        cos_full = col_ref[0] + row_ref[0, g : g + 1, :]
        sin_full = col_ref[1] + row_ref[1, g : g + 1, :]
        out_ref[span, :] = norm_rotate(k_ref[span, :], gain, cos_full, sin_full)
    copies[3].wait()


def query_kernel(
    q_hbm, ids_hbm, doc_hbm, gain_hbm, row_ref, col_ref, out_ref, qdoc_ref, slot_ref,
    q_ref, ids_ref, doc_ref, gain_ref, sems, *, capacity,
):
    copies = [
        pltpu.make_async_copy(src, dst, sems.at[n])
        for n, (src, dst) in enumerate(
            [(q_hbm, q_ref), (gain_hbm, gain_ref), (doc_hbm, doc_ref), (ids_hbm, ids_ref)]
        )
    ]
    for copy in copies:
        copy.start()
    for copy in copies:
        copy.wait()
    rows, width = q_ref.shape
    gain = gain_ref[...]
    for g in range(rows // GRID_W):
        span = slice(g * GRID_W, (g + 1) * GRID_W)
        cos_full = col_ref[0] + row_ref[0, g : g + 1, :]
        sin_full = col_ref[1] + row_ref[1, g : g + 1, :]
        for h in range(width // HEAD):
            lanes = slice(h * HEAD, (h + 1) * HEAD)
            out_ref[span, lanes] = norm_rotate(q_ref[span, lanes], gain, cos_full, sin_full)
    for t in range(doc_ref.shape[0]):
        line = jnp.broadcast_to(doc_ref[t : t + 1, :].astype(jnp.float32) + 1.0, (HEAD, HEAD))
        qdoc_ref[t * HEAD : (t + 1) * HEAD, :] = line.T
    choices, tokens = ids_ref.shape
    sub = lax.broadcasted_iota(jnp.int32, (HEAD, tokens), 0)
    lane = lax.broadcasted_iota(jnp.int32, (tokens, tokens), 1)
    upper = (lax.broadcasted_iota(jnp.int32, (tokens, tokens), 0) <= lane).astype(jnp.float32)
    upper = upper.astype(jnp.bfloat16)
    before = jnp.zeros((HEAD, 1), jnp.float32)
    for k in range(choices):
        ids = ids_ref[k : k + 1, :]
        hit = (sub == ids).astype(jnp.float32)
        running = before + jnp.dot(
            hit.astype(jnp.bfloat16), upper, preferred_element_type=jnp.float32
        )
        arrival = jnp.sum(running * hit, axis=0, keepdims=True) - 1.0
        slot_ref[k : k + 1, :] = ids * capacity + arrival.astype(jnp.int32)
        before = before + jnp.sum(hit, axis=1, keepdims=True)


def attend(
    quarters, edge_ref, q_ref, qdoc_ref, sources, state, out_refs,
    k_ref, v_ref, d_ref, list_ref, s_even, s_odd, mx_even, mx_odd, l_scr, acc_scr,
):
    rows, width = q_ref.shape
    heads = width // HEAD
    tiles = rows // HEAD
    block = rows // 4
    pieces = block // 16
    total = len(quarters)
    scale = HEAD ** (-0.5) * 1.4426950408889634
    spans = []
    for n, src in enumerate(sources):
        k_ref[n] = src[0:rows, :]
        v_ref[n] = src[rows : 2 * rows, :]
        docs = src[2 * rows : 2 * rows + DOC_ROWS, :].astype(jnp.float32)
        for t in range(tiles):
            d_ref[n * tiles + t] = jnp.broadcast_to(docs[t : t + 1, :], (8, HEAD))
        spans.append((jnp.min(docs[0:1, :]), jnp.max(docs[tiles - 1 : tiles, :])))
    counts = []
    for n, qs in enumerate(quarters):
        first = edge_ref[qs, 0].astype(jnp.float32) + 1.0
        last = edge_ref[qs, block - 1].astype(jnp.float32) + 1.0
        count = jnp.int32(0)
        for m in range(len(sources) + 1):
            list_ref[n, m] = 0
        for m, (low, high) in enumerate(spans):
            list_ref[n, count] = m
            count = count + ((low <= last) & (high >= first)).astype(jnp.int32)
        counts.append(count)
    s_refs = (s_even, s_odd)
    mx_refs = (mx_even, mx_odd)
    spare = len(sources)
    for ref in s_refs:
        ref[spare] = jnp.full(ref.shape[1:], LOW, jnp.float32)

    def scores(n, i):
        s_ref, mx_ref = s_refs[n % 2], mx_refs[n % 2]
        slot = list_ref[n, i]
        index = jnp.where(i < counts[n], i, spare + 1)

        def line(r):
            return pl.ds(pl.multiple_of(quarters[n] * block + r * 16, 16), 16)

        q4 = jnp.concatenate(
            [
                q_ref[line(r), h * HEAD : (h + 1) * HEAD]
                for r in range(pieces)
                for h in range(heads)
            ],
            0,
        )
        s = lax.dot_general(
            q4, k_ref[slot], (((1,), (1,)), ((), ())), preferred_element_type=jnp.float32
        )
        key_docs = [d_ref[slot * tiles + t] for t in range(tiles)]
        key_docs = [jnp.concatenate([d, d], 0) for d in key_docs]
        for r in range(pieces):
            qdoc = qdoc_ref[line(r), :]
            keep = [qdoc == d for d in key_docs]
            for h in range(heads):
                band = slice((r * heads + h) * 16, (r * heads + h + 1) * 16)
                top = mx_ref[band, :]
                for t in range(tiles):
                    lanes = slice(t * HEAD, (t + 1) * HEAD)
                    part = jnp.where(keep[t], s[band, lanes], LOW)
                    s_ref[index, band, lanes] = part
                    top = jnp.maximum(top, part)
                mx_ref[band, :] = top

    def weigh(n, i):
        s_ref, mx_ref = s_refs[n % 2], mx_refs[n % 2]
        slot = list_ref[n, i]
        index = jnp.where(i < counts[n], i, spare)
        top = mx_ref[...]
        probs = []
        run = l_scr[...]
        for t in range(tiles):
            e = jnp.exp2(s_ref[index, :, t * HEAD : (t + 1) * HEAD] * scale - top)
            run = run + e
            probs.append(e.astype(jnp.bfloat16))
        l_scr[...] = run
        acc_scr[...] += jnp.dot(
            jnp.concatenate(probs, axis=1), v_ref[slot], preferred_element_type=jnp.float32
        )

    m_ref, l_ref, acc_ref = state
    for step in range(total + 1):
        trip = counts[step] if step == 0 else counts[step - 1]
        if 0 < step < total:
            trip = jnp.maximum(trip, counts[step])
        if step < total:
            if out_refs is None:
                mx_refs[step % 2][...] = jnp.full(mx_even.shape, LOW, jnp.float32)
            else:
                mx_refs[step % 2][...] = m_ref[quarters[step]]
        if step > 0:
            if out_refs is None:
                l_scr[...] = jnp.zeros(l_scr.shape, jnp.float32)
                acc_scr[...] = jnp.zeros(acc_scr.shape, jnp.float32)
            else:
                before = quarters[step - 1]
                shrink = jnp.exp2(m_ref[before] * scale - mx_refs[(step - 1) % 2][...])
                l_scr[...] = l_ref[before] * shrink
                acc_scr[...] = acc_ref[before] * shrink

        def body(i, carry, step=step):
            if step > 0:
                weigh(step - 1, i)
            if step < total:
                scores(step, i)
            return carry

        lax.fori_loop(0, trip, body, 0)
        if step < total:
            ref = mx_refs[step % 2]
            top = jnp.broadcast_to(jnp.max(ref[...], axis=1, keepdims=True), ref.shape)
            if out_refs is None:
                m_ref[quarters[step]] = top
            ref[...] = top * scale
        if step > 0 and out_refs is None:
            l_ref[quarters[step - 1]] = l_scr[...]
            acc_ref[quarters[step - 1]] = acc_scr[...]
        elif step > 0:
            den = jnp.sum(l_scr[...], axis=1, keepdims=True)
            res = (acc_scr[...] / den).astype(jnp.bfloat16)
            for r in range(pieces):
                for h in range(heads):
                    at = (r * heads + h) * 16
                    out_refs[step - 1][r * 16 : (r + 1) * 16, h * HEAD : (h + 1) * HEAD] = res[
                        at : at + 16, :
                    ]


def early_attention(
    edge_ref, w_hbm, q_ref, qdoc_ref, own, near, b1, b3, m_ref, l_ref, acc_ref, w_ref, *scratch
):
    fetch = pltpu.make_async_copy(w_hbm, w_ref, scratch[-1])
    fetch.start()
    state = (m_ref, l_ref, acc_ref)
    sources = (own, near, b1, b3)
    attend(range(4), edge_ref, q_ref, qdoc_ref, sources, state, None, *scratch[:-1])
    fetch.wait()


def late_attention(
    where_ref, edge_ref, q_ref, qdoc_ref, b2, b4, far, m_ref, l_ref, acc_ref, out_a, out_b,
    *scratch, ahead,
):
    quarters = [(where_ref[1] + k) % 4 for k in ahead]
    state = (m_ref, l_ref, acc_ref)
    sources = (b2, b4, far)
    attend(quarters, edge_ref, q_ref, qdoc_ref, sources, state, (out_a, out_b), *scratch)


def weight_rows(w_ref, group, part):
    return w_ref[pl.ds(pl.multiple_of(group * part, part), part), :]


def project_part_kernel(where_ref, h0_ref, h2_ref, h3_ref, w_ref, acc_ref):
    part = h0_ref.shape[1]
    home = where_ref[1]
    acc = jnp.dot(h0_ref[...], weight_rows(w_ref, home, part), preferred_element_type=jnp.float32)
    for ref, back in ((h2_ref, 2), (h3_ref, 3)):
        acc += jnp.dot(
            ref[...], weight_rows(w_ref, (home + 4 - back) % 4, part),
            preferred_element_type=jnp.float32,
        )
    acc_ref[...] = acc


def project_kernel(
    where_ref, slot_ref, h1_ref, acc_ref, w_ref, res_ref, gain_ref, hid_ref, out_ref, n_scr
):
    rows, width = res_ref.shape
    fold = width // HEAD
    acc = acc_ref[...] + jnp.dot(
        h1_ref[...], weight_rows(w_ref, (where_ref[1] + 3) % 4, h1_ref.shape[1]),
        preferred_element_type=jnp.float32,
    )
    hidden = (res_ref[...].astype(jnp.float32) + acc).astype(jnp.bfloat16)
    hid_ref[...] = hidden
    wide = hidden.astype(jnp.float32)
    mean = jnp.mean(wide * wide, axis=-1, keepdims=True)
    normed = wide * lax.rsqrt(mean + norm_eps) * gain_ref[...]
    for c in range(fold):
        n_scr[pl.ds(c, rows, stride=fold), :] = normed[:, c * HEAD : (c + 1) * HEAD]
    zero = jnp.zeros((32,) + out_ref.shape[1:], jnp.bfloat16)
    for b in range(out_ref.shape[0] // 32):
        out_ref[b * 32 : (b + 1) * 32] = zero

    def place(step, carry):
        for u in range(8):
            token = step * 8 + u
            tile = n_scr[pl.ds(pl.multiple_of(token * fold, fold), fold), :].astype(jnp.bfloat16)
            out_ref[slot_ref[0, token]] = tile
            out_ref[slot_ref[1, token]] = tile
        return carry

    lax.fori_loop(0, rows // 8, place, 0)


def expert_kernel(in_ref, gate_ref, up_ref, down_ref, out_ref, f_scr, x_scr):
    slots, fold, _ = in_ref.shape
    part = slots // 4
    for b in range(4):
        band = slice(b * part, (b + 1) * part)
        f_scr[b * part * fold : (b + 1) * part * fold, :] = (
            in_ref[band].astype(jnp.float32).reshape(part * fold, HEAD)
        )
        for c in range(fold):
            x_scr[band, c * HEAD : (c + 1) * HEAD] = f_scr[
                pl.ds(b * part * fold + c, part, stride=fold), :
            ].astype(jnp.bfloat16)
    x = x_scr[...]
    gate = jnp.dot(x, gate_ref[0], preferred_element_type=jnp.float32)
    up = jnp.dot(x, up_ref[0], preferred_element_type=jnp.float32)
    act = (jax.nn.silu(gate) * up).astype(jnp.bfloat16)
    step = 2
    for n in range(fold // step):
        y = jnp.dot(
            act, down_ref[0, :, n * step * HEAD : (n + 1) * step * HEAD],
            preferred_element_type=jnp.float32,
        )
        for t in range(step):
            f_scr[pl.ds(n * step + t, slots, stride=fold), :] = y[:, t * HEAD : (t + 1) * HEAD]
    for b in range(4):
        out_ref[b * part : (b + 1) * part] = (
            f_scr[b * part * fold : (b + 1) * part * fold, :]
            .reshape(part, fold, HEAD)
            .astype(jnp.bfloat16)
        )


def combine_kernel(slot_ref, weight_ref, ret_ref, hid_ref, out_ref, c_scr):
    rows, width = hid_ref.shape
    fold = width // HEAD

    def gather(step, carry):
        for u in range(8):
            token = step * 8 + u
            one = ret_ref[slot_ref[0, token]].astype(jnp.float32) * weight_ref[0, token]
            two = ret_ref[slot_ref[1, token]].astype(jnp.float32) * weight_ref[1, token]
            c_scr[pl.ds(pl.multiple_of(token * fold, fold), fold), :] = one + two
        return carry

    lax.fori_loop(0, rows // 8, gather, 0)
    for c in range(fold):
        lanes = slice(c * HEAD, (c + 1) * HEAD)
        out_ref[:, lanes] = (
            hid_ref[:, lanes].astype(jnp.float32) + c_scr[pl.ds(c, rows, stride=fold), :]
        ).astype(jnp.bfloat16)


def in_hbm(x):
    return pltpu.with_memory_space_constraint(x, pltpu.HBM)


def call(kernel, out_shape, limit, scratch=(), smem=0, args=(), hbm=0):
    specs = [pl.BlockSpec(memory_space=pltpu.SMEM)] * smem
    specs += [pl.BlockSpec(memory_space=pltpu.HBM)] * hbm
    specs += [pl.BlockSpec(memory_space=VMEM)] * (len(args) - smem - hbm)
    return pl.pallas_call(
        kernel,
        out_shape=out_shape,
        in_specs=specs,
        out_specs=jax.tree.map(lambda _: pl.BlockSpec(memory_space=VMEM), out_shape),
        scratch_shapes=list(scratch),
        compiler_params=pltpu.CompilerParams(vmem_limit_bytes=limit * 2**20),
    )(*args)


def on_device(
    residual, query_proj, key_proj, value_proj, query_gain, key_gain, document_ids,
    output_weight, norm_gain, expert_ids, route_weights, gate_weight, up_weight, down_weight,
):
    bf16, f32 = jnp.bfloat16, jnp.float32
    sp = lax.axis_size("sp")
    index = lax.axis_index("sp")
    rows = query_proj.shape[0]
    row_tab, col_tab = rotary_tables(index * rows, rows)
    doc_lines = document_ids.reshape(rows // HEAD, HEAD)
    packed = pl.pallas_call(
        key_kernel,
        out_shape=jax.ShapeDtypeStruct((2 * rows + DOC_ROWS, HEAD), bf16),
        in_specs=[pl.BlockSpec(memory_space=pltpu.HBM)] * 4
        + [pl.BlockSpec(memory_space=VMEM)] * 2,
        out_specs=pl.BlockSpec(memory_space=VMEM),
        scratch_shapes=[
            VMEM((rows, HEAD), bf16),
            VMEM((rows // HEAD, HEAD), jnp.int32),
            VMEM((1, HEAD), f32),
            pltpu.SemaphoreType.DMA((4,)),
        ],
        name="key_prep",
        compiler_params=pltpu.CompilerParams(vmem_limit_bytes=8 * 2**20),
    )(
        in_hbm(key_proj), in_hbm(value_proj), in_hbm(doc_lines),
        in_hbm(key_gain.reshape(1, HEAD)), row_tab, col_tab,
    )
    swap = [(i, i ^ 1) for i in range(sp)]
    cross = [(i, (i + 1) % sp) if i % 2 else (i, (i - 1) % sp) for i in range(sp)]
    right = [(i, (i + 2) % sp) for i in range(sp)]
    left = [(i, (i - 2) % sp) for i in range(sp)]
    par = index % 2
    from_left = lax.ppermute(packed, "sp", right)
    from_right = lax.ppermute(packed, "sp", left)
    near = lax.ppermute(packed, "sp", swap)
    far = lax.ppermute(jnp.where(par == 1, from_left, from_right), "sp", cross)
    left_pair = lax.ppermute(from_left, "sp", swap)
    right_pair = lax.ppermute(from_right, "sp", swap)

    quarter = rows // 4
    width = query_proj.shape[1]
    token_rows, wide = residual.shape
    fold = wide // HEAD
    top_count = expert_ids.shape[1]
    experts_all = sp * lax.axis_size("tp")
    capacity = max(2, 2 * token_rows * top_count // experts_all)
    slots = experts_all * capacity
    query_norm, query_doc, slot = call(
        functools.partial(query_kernel, capacity=capacity),
        (
            jax.ShapeDtypeStruct(query_proj.shape, bf16),
            jax.ShapeDtypeStruct((rows, HEAD), f32),
            jax.ShapeDtypeStruct((top_count, token_rows), jnp.int32),
        ),
        8,
        scratch=(
            VMEM(query_proj.shape, bf16),
            VMEM((top_count, token_rows), jnp.int32),
            VMEM(doc_lines.shape, jnp.int32),
            VMEM((1, HEAD), f32),
            pltpu.SemaphoreType.DMA((4,)),
        ),
        hbm=4,
        args=(
            in_hbm(query_proj), in_hbm(expert_ids.T), in_hbm(doc_lines),
            in_hbm(query_gain.reshape(1, HEAD)), row_tab, col_tab,
        ),
    )
    where = jnp.stack([par, lax.axis_index("tp")]).astype(jnp.int32)

    def attention_scratch(count):
        return (
            VMEM((count, rows, HEAD), bf16),
            VMEM((count, rows, HEAD), bf16),
            VMEM((count * rows // HEAD, 8, HEAD), f32),
            pltpu.SMEM((4, count + 1), jnp.int32),
            VMEM((count + 2, rows, rows), f32),
            VMEM((count + 2, rows, rows), f32),
            VMEM((rows, HEAD), f32),
            VMEM((rows, HEAD), f32),
            VMEM((rows, HEAD), f32),
            VMEM((rows, HEAD), f32),
        )

    part_shape = jax.ShapeDtypeStruct((quarter, width), bf16)
    state_shape = jax.ShapeDtypeStruct((4, rows, HEAD), f32)
    top, sums, values, weight_near = call(
        early_attention,
        (
            state_shape,
            state_shape,
            state_shape,
            jax.ShapeDtypeStruct(output_weight.shape, bf16),
        ),
        24,
        scratch=attention_scratch(4) + (pltpu.SemaphoreType.DMA,),
        smem=1,
        hbm=1,
        args=(
            doc_lines, in_hbm(output_weight), query_norm, query_doc, packed, near, from_left,
            from_right,
        ),
    )

    def late(ahead):
        return call(
            functools.partial(late_attention, ahead=ahead), (part_shape, part_shape), 24,
            scratch=attention_scratch(3), smem=2,
            args=(
                where, doc_lines, query_norm, query_doc, left_pair, right_pair, far, top, sums,
                values,
            ),
        )

    def ahead_by(x, k):
        return lax.ppermute(x, "tp", [(i, (i + k) % 4) for i in range(4)])

    ahead_2, ahead_3 = late((2, 3))
    heads_2 = ahead_by(ahead_2, 2)
    heads_3 = ahead_by(ahead_3, 3)
    ahead_1, at_home = late((1, 0))
    heads_1 = ahead_by(ahead_1, 1)
    partial = call(
        project_part_kernel, jax.ShapeDtypeStruct((token_rows, wide), f32), 16,
        smem=1, args=(where, at_home, heads_2, heads_3, weight_near),
    )
    hidden, outgoing = call(
        project_kernel,
        (
            jax.ShapeDtypeStruct((token_rows, wide), bf16),
            jax.ShapeDtypeStruct((slots, fold, HEAD), bf16),
        ),
        16,
        scratch=(VMEM((token_rows * fold, HEAD), f32),),
        smem=2,
        args=(where, slot, heads_1, partial, weight_near, residual, norm_gain.reshape(1, wide)),
    )

    def exchange(x):
        x = x.reshape(experts_all, capacity * fold, HEAD)
        x = lax.all_to_all(x, ("sp", "tp"), split_axis=0, concat_axis=0, tiled=True)
        return x.reshape(slots, fold, HEAD)

    arrived = exchange(outgoing)
    expert_out = call(
        expert_kernel,
        jax.ShapeDtypeStruct((slots, fold, HEAD), bf16),
        32,
        scratch=(VMEM((slots * fold, HEAD), f32), VMEM((slots, wide), bf16)),
        args=(arrived, gate_weight, up_weight, down_weight),
    )
    returned = exchange(expert_out)
    return call(
        combine_kernel,
        jax.ShapeDtypeStruct((token_rows, wide), bf16),
        16,
        scratch=(VMEM((token_rows * fold, HEAD), f32),),
        smem=2,
        args=(slot, route_weights.T, returned, hidden),
    )


def solution(mesh):
    both = P(("sp", "tp"), None)
    in_specs = (
        both, P("sp", "tp"), P("sp", "tp"), P("sp", "tp"), P(), P(), P("sp"), P(), P(),
        both, both,
        P(("sp", "tp"), None, None), P(("sp", "tp"), None, None), P(("sp", "tp"), None, None),
    )

    return jax.shard_map(on_device, mesh=mesh, in_specs=in_specs, out_specs=both, check_vma=False)
```

```python
import functools

import jax
import jax.numpy as jnp
from jax import lax
from jax.experimental import pallas as pl
from jax.experimental.pallas import tpu as pltpu
from jax.sharding import PartitionSpec as P


HEAD = 128
HALF = HEAD // 2
GRID_W = 64
norm_eps = 1e-06
rope_base = 10000.0
LOW = -1e30
DOC_ROWS = 16
VMEM = pltpu.VMEM


def rotary_tables(first_row, length):
    count = HEAD // 4
    inverse = 1.0 / rope_base ** (jnp.arange(count, dtype=jnp.float32) / count)
    rows = (first_row // GRID_W + jnp.arange(length // GRID_W, dtype=jnp.int32)).astype(jnp.float32)
    cols = jnp.arange(GRID_W, dtype=jnp.int32).astype(jnp.float32)
    row_angle = rows[:, None] * inverse[None, :]
    col_angle = cols[:, None] * inverse[None, :]
    rz = jnp.zeros_like(row_angle)
    cz = jnp.zeros_like(col_angle)
    rc, rs = jnp.cos(row_angle), jnp.sin(row_angle)
    cc, cs = jnp.cos(col_angle), jnp.sin(col_angle)
    row_tab = jnp.stack(
        [jnp.concatenate([rc, rz, rc, rz], 1), jnp.concatenate([-rs, rz, rs, rz], 1)]
    )
    col_tab = jnp.stack(
        [jnp.concatenate([cz, cc, cz, cc], 1), jnp.concatenate([cz, -cs, cz, cs], 1)]
    )
    return row_tab, col_tab


def norm_rotate(x, gain, cos_full, sin_full):
    wide = x.astype(jnp.float32)
    square = wide * wide
    high = square.astype(jnp.bfloat16)
    low = (square - high.astype(jnp.float32)).astype(jnp.bfloat16)
    ones = jnp.ones((HEAD, HEAD), jnp.bfloat16)
    mean = (
        jnp.dot(high, ones, preferred_element_type=jnp.float32)
        + jnp.dot(low, ones, preferred_element_type=jnp.float32)
    ) * (1.0 / HEAD)
    scaled = wide * lax.rsqrt(mean + norm_eps) * gain
    return (scaled * cos_full + pltpu.roll(scaled, HALF, 1) * sin_full).astype(jnp.bfloat16)


def key_kernel(
    k_hbm, v_hbm, doc_hbm, gain_hbm, row_ref, col_ref, out_ref, k_ref, doc_ref, gain_ref, sems
):
    rows = k_ref.shape[0]
    copies = [
        pltpu.make_async_copy(k_hbm, k_ref, sems.at[0]),
        pltpu.make_async_copy(gain_hbm, gain_ref, sems.at[1]),
        pltpu.make_async_copy(doc_hbm, doc_ref, sems.at[2]),
        pltpu.make_async_copy(v_hbm, out_ref.at[pl.ds(rows, rows), :], sems.at[3]),
    ]
    for copy in copies:
        copy.start()
    for copy in copies[:3]:
        copy.wait()
    docs = (doc_ref[...].astype(jnp.float32) + 1.0).astype(jnp.bfloat16)
    pad = jnp.zeros((DOC_ROWS - docs.shape[0], HEAD), jnp.bfloat16)
    out_ref[2 * rows :, :] = jnp.concatenate([docs, pad], 0)
    gain = gain_ref[...]
    for g in range(rows // GRID_W):
        span = slice(g * GRID_W, (g + 1) * GRID_W)
        cos_full = col_ref[0] + row_ref[0, g : g + 1, :]
        sin_full = col_ref[1] + row_ref[1, g : g + 1, :]
        out_ref[span, :] = norm_rotate(k_ref[span, :], gain, cos_full, sin_full)
    copies[3].wait()


def pick_kernel(edge_ref, left_ref, right_ref, out_ref):
    @pl.when(edge_ref[edge_ref.shape[0] - 2, 0] == 1)
    def _():
        out_ref[...] = left_ref[...]

    @pl.when(edge_ref[edge_ref.shape[0] - 2, 0] == 0)
    def _():
        out_ref[...] = right_ref[...]


def query_kernel(
    where_ref, q_hbm, ids_hbm, doc_hbm, gain_hbm, row_ref, col_ref, out_ref, qdoc_ref, slot_ref, edge_ref,
    q_ref, ids_ref, doc_ref, gain_ref, sems, *, capacity,
):
    copies = [
        pltpu.make_async_copy(src, dst, sems.at[n])
        for n, (src, dst) in enumerate(
            [(q_hbm, q_ref), (gain_hbm, gain_ref), (doc_hbm, doc_ref), (ids_hbm, ids_ref)]
        )
    ]
    for copy in copies:
        copy.start()
    for copy in copies:
        copy.wait()
    tiles = doc_ref.shape[0]
    edge_ref[0:tiles, :] = doc_ref[...]
    for n in range(2):
        edge_ref[tiles + n : tiles + n + 1, :] = jnp.full((1, HEAD), where_ref[n], jnp.int32)
    rows, width = q_ref.shape
    gain = gain_ref[...]
    for g in range(rows // GRID_W):
        span = slice(g * GRID_W, (g + 1) * GRID_W)
        cos_full = col_ref[0] + row_ref[0, g : g + 1, :]
        sin_full = col_ref[1] + row_ref[1, g : g + 1, :]
        for h in range(width // HEAD):
            lanes = slice(h * HEAD, (h + 1) * HEAD)
            out_ref[span, lanes] = norm_rotate(q_ref[span, lanes], gain, cos_full, sin_full)
    for t in range(doc_ref.shape[0]):
        line = jnp.broadcast_to(doc_ref[t : t + 1, :].astype(jnp.float32) + 1.0, (HEAD, HEAD))
        qdoc_ref[t * HEAD : (t + 1) * HEAD, :] = line.T
    choices, tokens = ids_ref.shape
    sub = lax.broadcasted_iota(jnp.int32, (HEAD, tokens), 0)
    lane = lax.broadcasted_iota(jnp.int32, (tokens, tokens), 1)
    upper = (lax.broadcasted_iota(jnp.int32, (tokens, tokens), 0) <= lane).astype(jnp.float32)
    upper = upper.astype(jnp.bfloat16)
    before = jnp.zeros((HEAD, 1), jnp.float32)
    for k in range(choices):
        ids = ids_ref[k : k + 1, :]
        hit = (sub == ids).astype(jnp.float32)
        running = before + jnp.dot(
            hit.astype(jnp.bfloat16), upper, preferred_element_type=jnp.float32
        )
        arrival = jnp.sum(running * hit, axis=0, keepdims=True) - 1.0
        slot_ref[k : k + 1, :] = ids * capacity + arrival.astype(jnp.int32)
        before = before + jnp.sum(hit, axis=1, keepdims=True)


def attend(
    quarters, edge_ref, q_ref, qdoc_ref, sources, state, store, out_refs,
    k_ref, v_ref, d_ref, list_ref, s_even, s_odd, mx_even, mx_odd, l_scr, acc_scr,
):
    rows, width = q_ref.shape
    heads = width // HEAD
    tiles = rows // HEAD
    block = rows // 4
    pieces = block // 16
    total = len(quarters)
    scale = HEAD ** (-0.5) * 1.4426950408889634
    spans = []
    for n, src in enumerate(sources):
        k_ref[n] = src[0:rows, :]
        v_ref[n] = src[rows : 2 * rows, :]
        docs = src[2 * rows : 2 * rows + DOC_ROWS, :].astype(jnp.float32)
        for t in range(tiles):
            d_ref[n * tiles + t] = jnp.broadcast_to(docs[t : t + 1, :], (8, HEAD))
        spans.append((jnp.min(docs[0:1, :]), jnp.max(docs[tiles - 1 : tiles, :])))
    counts = []
    for n, qs in enumerate(quarters):
        first = edge_ref[qs, 0].astype(jnp.float32) + 1.0
        last = edge_ref[qs, block - 1].astype(jnp.float32) + 1.0
        count = jnp.int32(0)
        for m in range(len(sources) + 1):
            list_ref[n, m] = 0
        for m, (low, high) in enumerate(spans):
            list_ref[n, count] = m
            count = count + ((low <= last) & (high >= first)).astype(jnp.int32)
        counts.append(count)
    s_refs = (s_even, s_odd)
    mx_refs = (mx_even, mx_odd)

    def scores(n, i):
        s_ref, mx_ref = s_refs[n % 2], mx_refs[n % 2]
        slot = list_ref[n, i]

        def line(r):
            return pl.ds(pl.multiple_of(quarters[n] * block + r * 16, 16), 16)

        q4 = jnp.concatenate(
            [
                q_ref[line(r), h * HEAD : (h + 1) * HEAD]
                for r in range(pieces)
                for h in range(heads)
            ],
            0,
        )
        s = lax.dot_general(
            q4, k_ref[slot], (((1,), (1,)), ((), ())), preferred_element_type=jnp.float32
        )
        key_docs = [d_ref[slot * tiles + t] for t in range(tiles)]
        key_docs = [jnp.concatenate([d, d], 0) for d in key_docs]
        for r in range(pieces):
            qdoc = qdoc_ref[line(r), :]
            keep = [qdoc == d for d in key_docs]
            for h in range(heads):
                band = slice((r * heads + h) * 16, (r * heads + h + 1) * 16)
                top = mx_ref[band, :]
                for t in range(tiles):
                    lanes = slice(t * HEAD, (t + 1) * HEAD)
                    part = jnp.where(keep[t], s[band, lanes], LOW)
                    s_ref[i, band, lanes] = part
                    top = jnp.maximum(top, part)
                mx_ref[band, :] = top

    def weigh(n, i):
        s_ref, mx_ref = s_refs[n % 2], mx_refs[n % 2]
        slot = list_ref[n, i]
        top = mx_ref[...]
        probs = []
        run = l_scr[...]
        for t in range(tiles):
            e = jnp.exp2(s_ref[i, :, t * HEAD : (t + 1) * HEAD] * scale - top)
            run = run + e
            probs.append(e.astype(jnp.bfloat16))
        l_scr[...] = run
        acc_scr[...] += jnp.dot(
            jnp.concatenate(probs, axis=1), v_ref[slot], preferred_element_type=jnp.float32
        )

    m_ref, l_ref, acc_ref = state or (None,) * 3
    for step in range(total + 1):
        if step < total:
            if state is None:
                mx_refs[step % 2][...] = jnp.full(mx_even.shape, LOW, jnp.float32)
            else:
                mx_refs[step % 2][...] = m_ref[quarters[step]]
        if step > 0:
            if state is None:
                l_scr[...] = jnp.zeros(l_scr.shape, jnp.float32)
                acc_scr[...] = jnp.zeros(acc_scr.shape, jnp.float32)
            else:
                before = quarters[step - 1]
                shrink = jnp.exp2(m_ref[before] * scale - mx_refs[(step - 1) % 2][...])
                l_scr[...] = l_ref[before] * shrink
                acc_scr[...] = acc_ref[before] * shrink

        def both(i, carry, step=step):
            weigh(step - 1, i)
            scores(step, i)
            return carry

        def behind(i, carry, step=step):
            weigh(step - 1, i)
            return carry

        def ahead(i, carry, step=step):
            scores(step, i)
            return carry

        shared = 0
        if 0 < step < total:
            shared = jnp.minimum(counts[step - 1], counts[step])
            lax.fori_loop(0, shared, both, 0)
        if step > 0:
            lax.fori_loop(shared, counts[step - 1], behind, 0)
        if step < total:
            lax.fori_loop(shared, counts[step], ahead, 0)
        if step < total:
            ref = mx_refs[step % 2]
            top = jnp.broadcast_to(jnp.max(ref[...], axis=1, keepdims=True), ref.shape)
            if store is not None:
                store[0][quarters[step]] = top
            ref[...] = top * scale
        if step > 0 and store is not None:
            store[1][quarters[step - 1]] = l_scr[...]
            store[2][quarters[step - 1]] = acc_scr[...]
        elif step > 0:
            den = jnp.sum(l_scr[...], axis=1, keepdims=True)
            res = (acc_scr[...] / den).astype(jnp.bfloat16)
            for r in range(pieces):
                for h in range(heads):
                    at = (r * heads + h) * 16
                    out_refs[step - 1][r * 16 : (r + 1) * 16, h * HEAD : (h + 1) * HEAD] = res[
                        at : at + 16, :
                    ]


def home_attention(edge_ref, w_hbm, q_ref, qdoc_ref, own, near, m_ref, l_ref, acc_ref, w_ref, *scratch):
    fetch = pltpu.make_async_copy(w_hbm, w_ref, scratch[-1])
    fetch.start()
    store = (m_ref, l_ref, acc_ref)
    attend(range(4), edge_ref, q_ref, qdoc_ref, (own, near), None, store, None, *scratch[:-1])
    fetch.wait()


def early_attention(
    edge_ref, q_ref, qdoc_ref, b1, b3, m_in, l_in, acc_in, m_ref, l_ref, acc_ref, *scratch
):
    state, store = (m_in, l_in, acc_in), (m_ref, l_ref, acc_ref)
    attend(range(4), edge_ref, q_ref, qdoc_ref, (b1, b3), state, store, None, *scratch)


def home_index(edge_ref):
    return edge_ref[edge_ref.shape[0] - 1, 0]


def late_attention(
    edge_ref, q_ref, qdoc_ref, b2, b4, far, m_ref, l_ref, acc_ref, out_a, out_b,
    *scratch, ahead,
):
    quarters = [(home_index(edge_ref) + k) % 4 for k in ahead]
    state = (m_ref, l_ref, acc_ref)
    sources = (b2, b4, far)
    attend(quarters, edge_ref, q_ref, qdoc_ref, sources, state, None, (out_a, out_b), *scratch)


def weight_rows(w_ref, group, part):
    return w_ref[pl.ds(pl.multiple_of(group * part, part), part), :]


def project_part_kernel(edge_ref, h0_ref, h2_ref, h3_ref, w_ref, acc_ref):
    part = h0_ref.shape[1]
    home = home_index(edge_ref)
    acc = jnp.dot(h0_ref[...], weight_rows(w_ref, home, part), preferred_element_type=jnp.float32)
    for ref, back in ((h2_ref, 2), (h3_ref, 3)):
        acc += jnp.dot(
            ref[...], weight_rows(w_ref, (home + 4 - back) % 4, part),
            preferred_element_type=jnp.float32,
        )
    acc_ref[...] = acc


def project_kernel(
    edge_ref, slot_ref, h1_ref, acc_ref, w_ref, res_ref, gain_ref, hid_ref, out_ref, n_scr
):
    rows, width = res_ref.shape
    fold = width // HEAD
    acc = acc_ref[...] + jnp.dot(
        h1_ref[...], weight_rows(w_ref, (home_index(edge_ref) + 3) % 4, h1_ref.shape[1]),
        preferred_element_type=jnp.float32,
    )
    hidden = (res_ref[...].astype(jnp.float32) + acc).astype(jnp.bfloat16)
    hid_ref[...] = hidden
    wide = hidden.astype(jnp.float32)
    mean = jnp.mean(wide * wide, axis=-1, keepdims=True)
    normed = wide * lax.rsqrt(mean + norm_eps) * gain_ref[...]
    for c in range(fold):
        n_scr[pl.ds(c, rows, stride=fold), :] = normed[:, c * HEAD : (c + 1) * HEAD]

    def place(step, carry):
        for u in range(8):
            token = step * 8 + u
            tile = n_scr[pl.ds(pl.multiple_of(token * fold, fold), fold), :].astype(jnp.bfloat16)
            out_ref[slot_ref[0, token]] = tile
            out_ref[slot_ref[1, token]] = tile
        return carry

    lax.fori_loop(0, rows // 8, place, 0)


def expert_kernel(in_ref, gate_ref, up_ref, down_ref, out_ref, f_scr, x_scr):
    slots, fold, _ = in_ref.shape
    part = slots // 4
    for b in range(4):
        band = slice(b * part, (b + 1) * part)
        f_scr[b * part * fold : (b + 1) * part * fold, :] = (
            in_ref[band].astype(jnp.float32).reshape(part * fold, HEAD)
        )
        for c in range(fold):
            x_scr[band, c * HEAD : (c + 1) * HEAD] = f_scr[
                pl.ds(b * part * fold + c, part, stride=fold), :
            ].astype(jnp.bfloat16)
    x = x_scr[...]
    gate = jnp.dot(x, gate_ref[0], preferred_element_type=jnp.float32)
    up = jnp.dot(x, up_ref[0], preferred_element_type=jnp.float32)
    act = (jax.nn.silu(gate) * up).astype(jnp.bfloat16)
    step = 2
    for n in range(fold // step):
        y = jnp.dot(
            act, down_ref[0, :, n * step * HEAD : (n + 1) * step * HEAD],
            preferred_element_type=jnp.float32,
        )
        for t in range(step):
            f_scr[pl.ds(n * step + t, slots, stride=fold), :] = y[:, t * HEAD : (t + 1) * HEAD]
    for b in range(4):
        out_ref[b * part : (b + 1) * part] = (
            f_scr[b * part * fold : (b + 1) * part * fold, :]
            .reshape(part, fold, HEAD)
            .astype(jnp.bfloat16)
        )


def combine_kernel(slot_ref, weight_ref, ret_ref, hid_ref, out_ref, c_scr):
    rows, width = hid_ref.shape
    fold = width // HEAD

    def gather(step, carry):
        for u in range(8):
            token = step * 8 + u
            one = ret_ref[slot_ref[0, token]].astype(jnp.float32) * weight_ref[0, token]
            two = ret_ref[slot_ref[1, token]].astype(jnp.float32) * weight_ref[1, token]
            c_scr[pl.ds(pl.multiple_of(token * fold, fold), fold), :] = one + two
        return carry

    lax.fori_loop(0, rows // 8, gather, 0)
    for c in range(fold):
        lanes = slice(c * HEAD, (c + 1) * HEAD)
        out_ref[:, lanes] = (
            hid_ref[:, lanes].astype(jnp.float32) + c_scr[pl.ds(c, rows, stride=fold), :]
        ).astype(jnp.bfloat16)


def in_hbm(x):
    return pltpu.with_memory_space_constraint(x, pltpu.HBM)


def call(kernel, out_shape, limit, scratch=(), smem=0, args=(), hbm=0):
    specs = [pl.BlockSpec(memory_space=pltpu.SMEM)] * smem
    specs += [pl.BlockSpec(memory_space=pltpu.HBM)] * hbm
    specs += [pl.BlockSpec(memory_space=VMEM)] * (len(args) - smem - hbm)
    return pl.pallas_call(
        kernel,
        out_shape=out_shape,
        in_specs=specs,
        out_specs=jax.tree.map(lambda _: pl.BlockSpec(memory_space=VMEM), out_shape),
        scratch_shapes=list(scratch),
        compiler_params=pltpu.CompilerParams(vmem_limit_bytes=limit * 2**20),
    )(*args)


def on_device(
    residual, query_proj, key_proj, value_proj, query_gain, key_gain, document_ids,
    output_weight, norm_gain, expert_ids, route_weights, gate_weight, up_weight, down_weight,
):
    bf16, f32 = jnp.bfloat16, jnp.float32
    sp = lax.axis_size("sp")
    index = lax.axis_index("sp")
    rows = query_proj.shape[0]
    row_tab, col_tab = rotary_tables(index * rows, rows)
    doc_lines = document_ids.reshape(rows // HEAD, HEAD)
    packed = pl.pallas_call(
        key_kernel,
        out_shape=jax.ShapeDtypeStruct((2 * rows + DOC_ROWS, HEAD), bf16),
        in_specs=[pl.BlockSpec(memory_space=pltpu.HBM)] * 4
        + [pl.BlockSpec(memory_space=VMEM)] * 2,
        out_specs=pl.BlockSpec(memory_space=VMEM),
        scratch_shapes=[
            VMEM((rows, HEAD), bf16),
            VMEM((rows // HEAD, HEAD), jnp.int32),
            VMEM((1, HEAD), f32),
            pltpu.SemaphoreType.DMA((4,)),
        ],
        name="key_prep",
        compiler_params=pltpu.CompilerParams(vmem_limit_bytes=8 * 2**20),
    )(
        in_hbm(key_proj), in_hbm(value_proj), in_hbm(doc_lines),
        in_hbm(key_gain.reshape(1, HEAD)), row_tab, col_tab,
    )
    swap = [(i, i ^ 1) for i in range(sp)]
    cross = [(i, (i + 1) % sp) if i % 2 else (i, (i - 1) % sp) for i in range(sp)]
    right = [(i, (i + 2) % sp) for i in range(sp)]
    left = [(i, (i - 2) % sp) for i in range(sp)]
    par = index % 2
    from_left = lax.ppermute(packed, "sp", right)
    from_right = lax.ppermute(packed, "sp", left)
    near = lax.ppermute(packed, "sp", swap)

    quarter = rows // 4
    width = query_proj.shape[1]
    token_rows, wide = residual.shape
    fold = wide // HEAD
    top_count = expert_ids.shape[1]
    experts_all = sp * lax.axis_size("tp")
    capacity = max(2, 2 * token_rows * top_count // experts_all)
    slots = experts_all * capacity
    query_norm, query_doc, slot, edges = call(
        functools.partial(query_kernel, capacity=capacity),
        (
            jax.ShapeDtypeStruct(query_proj.shape, bf16),
            jax.ShapeDtypeStruct((rows, HEAD), f32),
            jax.ShapeDtypeStruct((top_count, token_rows), jnp.int32),
            jax.ShapeDtypeStruct((doc_lines.shape[0] + 2, HEAD), jnp.int32),
        ),
        8,
        scratch=(
            VMEM(query_proj.shape, bf16),
            VMEM((top_count, token_rows), jnp.int32),
            VMEM(doc_lines.shape, jnp.int32),
            VMEM((1, HEAD), f32),
            pltpu.SemaphoreType.DMA((4,)),
        ),
        smem=1,
        hbm=4,
        args=(
            jnp.stack([par, lax.axis_index("tp")]).astype(jnp.int32), in_hbm(query_proj), in_hbm(expert_ids.T), in_hbm(doc_lines),
            in_hbm(query_gain.reshape(1, HEAD)), row_tab, col_tab,
        ),
    )
    passed = call(
        pick_kernel, jax.ShapeDtypeStruct(packed.shape, bf16), 4, smem=1,
        args=(edges, from_left, from_right),
    )
    far = lax.ppermute(passed, "sp", cross)
    left_pair = lax.ppermute(from_left, "sp", swap)
    right_pair = lax.ppermute(from_right, "sp", swap)

    def attention_scratch(count):
        return (
            VMEM((count, rows, HEAD), bf16),
            VMEM((count, rows, HEAD), bf16),
            VMEM((count * rows // HEAD, 8, HEAD), f32),
            pltpu.SMEM((4, count + 1), jnp.int32),
            VMEM((count, rows, rows), f32),
            VMEM((count, rows, rows), f32),
            VMEM((rows, HEAD), f32),
            VMEM((rows, HEAD), f32),
            VMEM((rows, HEAD), f32),
            VMEM((rows, HEAD), f32),
        )

    part_shape = jax.ShapeDtypeStruct((quarter, width), bf16)
    state_shape = jax.ShapeDtypeStruct((4, rows, HEAD), f32)
    top, sums, values, weight_near = call(
        home_attention,
        (
            state_shape,
            state_shape,
            state_shape,
            jax.ShapeDtypeStruct(output_weight.shape, bf16),
        ),
        24,
        scratch=attention_scratch(2) + (pltpu.SemaphoreType.DMA,),
        smem=1,
        hbm=1,
        args=(edges, in_hbm(output_weight), query_norm, query_doc, packed, near),
    )
    top, sums, values = call(
        early_attention, (state_shape, state_shape, state_shape), 24,
        scratch=attention_scratch(2),
        smem=1,
        args=(edges, query_norm, query_doc, from_left, from_right, top, sums, values),
    )

    def late(ahead):
        return call(
            functools.partial(late_attention, ahead=ahead), (part_shape, part_shape), 24,
            scratch=attention_scratch(3), smem=1,
            args=(
                edges, query_norm, query_doc, left_pair, right_pair, far, top, sums,
                values,
            ),
        )

    def ahead_by(x, k):
        return lax.ppermute(x, "tp", [(i, (i + k) % 4) for i in range(4)])

    ahead_2, ahead_3 = late((2, 3))
    heads_2 = ahead_by(ahead_2, 2)
    heads_3 = ahead_by(ahead_3, 3)
    ahead_1, at_home = late((1, 0))
    heads_1 = ahead_by(ahead_1, 1)
    partial = call(
        project_part_kernel, jax.ShapeDtypeStruct((token_rows, wide), f32), 16,
        smem=1, args=(edges, at_home, heads_2, heads_3, weight_near),
    )
    hidden, outgoing = call(
        project_kernel,
        (
            jax.ShapeDtypeStruct((token_rows, wide), bf16),
            jax.ShapeDtypeStruct((slots, fold, HEAD), bf16),
        ),
        16,
        scratch=(VMEM((token_rows * fold, HEAD), f32),),
        smem=2,
        args=(edges, slot, heads_1, partial, weight_near, residual, norm_gain.reshape(1, wide)),
    )

    def exchange(x):
        x = x.reshape(experts_all, capacity * fold, HEAD)
        x = lax.all_to_all(x, ("sp", "tp"), split_axis=0, concat_axis=0, tiled=True)
        return x.reshape(slots, fold, HEAD)

    arrived = exchange(outgoing)
    expert_out = call(
        expert_kernel,
        jax.ShapeDtypeStruct((slots, fold, HEAD), bf16),
        32,
        scratch=(VMEM((slots * fold, HEAD), f32), VMEM((slots, wide), bf16)),
        args=(arrived, gate_weight, up_weight, down_weight),
    )
    returned = exchange(expert_out)
    return call(
        combine_kernel,
        jax.ShapeDtypeStruct((token_rows, wide), bf16),
        16,
        scratch=(VMEM((token_rows * fold, HEAD), f32),),
        smem=2,
        args=(slot, route_weights.T, returned, hidden),
    )


def solution(mesh):
    both = P(("sp", "tp"), None)
    in_specs = (
        both, P("sp", "tp"), P("sp", "tp"), P("sp", "tp"), P(), P(), P("sp"), P(), P(),
        both, both,
        P(("sp", "tp"), None, None), P(("sp", "tp"), None, None), P(("sp", "tp"), None, None),
    )

    return jax.shard_map(on_device, mesh=mesh, in_specs=in_specs, out_specs=both, check_vma=False)
```
